32 devices in a mesh: tp: 32 (over z, y, x, core).
Axes of the slice: x: 2, y: 2, z: 4, core: 2. Of those that a mesh axis runs over, the one named last changes fastest.
Arguments:
- tokens: bfloat16 [32, 4096], replicated, may hold values from -18 to 18
- norm_gain: float32 [2, 4096], replicated, may hold values from 0.1 to 1.9
- w_gate: bfloat16 [2, 4096, 8192], P(None, None, 'tp'), may hold values from -0.09375 to 0.09375
- w_value: bfloat16 [2, 4096, 8192], P(None, None, 'tp'), may hold values from -0.09375 to 0.09375
- w_write: bfloat16 [2, 4096, 1024], P(None, None, 'tp'), may hold values from -0.09375 to 0.09375
- w_read: bfloat16 [2, 4096, 1024], P(None, None, 'tp'), may hold values from -0.09375 to 0.09375
- w_step: bfloat16 [2, 4096, 128], replicated, may hold values from -0.09375 to 0.09375
- step_bias: float32 [2, 128], replicated, may hold values from -2 to 1
- decay_rate: float32 [2, 128], replicated, may hold values from 0.05 to 3
- skip_gain: float32 [2, 128], replicated, may hold values from 1 to 4
- conv_value_weight: float32 [2, 3, 8192], P(None, None, 'tp'), may hold values from -2.5 to 2.5
- conv_key_weight: float32 [2, 3, 2, 1024], P(None, None, None, 'tp'), may hold values from -2.5 to 2.5
- group_gain: float32 [2, 8192], P(None, 'tp'), may hold values from 0.1 to 1.9
- w_out: bfloat16 [2, 8192, 4096], P(None, 'tp'), may hold values from -0.0625 to 0.0625
- ssm_state: float32 [2, 32, 8192, 128], P(None, None, 'tp'), may hold values from -3 to 3
- conv_value: float32 [2, 32, 2, 8192], P(None, None, None, 'tp'), may hold values from -5 to 5
- conv_key: float32 [2, 32, 2, 2, 1024], P(None, None, None, None, 'tp'), may hold values from -5 to 5
Outputs:
- tokens_out: bfloat16 [32, 4096], replicated
- ssm_state_out: float32 [2, 32, 8192, 128], P(None, None, 'tp')
- conv_value_out: float32 [2, 32, 2, 8192], P(None, None, None, 'tp')
- conv_key_out: float32 [2, 32, 2, 2, 1024], P(None, None, None, None, 'tp')
The draws below stay inside these ranges and needn't reach their ends.
All inputs are finite; a program needn't handle non-finite values.
Results may differ from the reference program's by a relative error of at most 0.011.
Values may be sent and summed in bfloat16 or wider, within the bound.
A program may use at most 128 MiB of HBM per device.

```python
import math
import jax
import jax.numpy as jnp
from jax import lax

D = 4096
SSDW = 8192
HEAD_DIM = 64
GROUPS = 8
STATE = 128
CONV = 3
LAYERS = 2
BATCH = 32
HEADS = 128
HPG = 16
GW = 1024


def draw_tokens(key, part):
    key_scale, key_value = jax.random.split(key)
    column_scale = jnp.exp(jax.random.uniform(key_scale, (1, D), jnp.float32, math.log(0.3), math.log(3.0)))
    values = jnp.clip(jax.random.normal(key_value, (BATCH, D), jnp.float32), -6.0, 6.0)
    return (values * column_scale).astype(jnp.bfloat16)


def levels(stream_key, dims, cuts, smallest, high):
    gain, own = 1.0, jax.random.fold_in(stream_key, 6)
    for axis_at, shards_of in cuts:
        heights = jnp.exp(jax.random.uniform(jax.random.fold_in(own, axis_at), (shards_of,), jnp.float32, smallest / len(cuts), high / len(cuts)))
        gain = gain * jnp.repeat(heights, dims[axis_at] // shards_of).reshape([-1 if axis == axis_at else 1 for axis in range(len(dims))])
    return gain


def noise(own_key, shape, deviation, most, pieces=(), kind=jnp.bfloat16):
    result = deviation * jax.random.normal(own_key, shape, jnp.float32)
    if pieces:
        result = result * levels(own_key, shape, pieces, -0.22, 0.18)
    return jnp.clip(result, -most, most).astype(kind)


def setup_inputs(seed: int = 0) -> dict:
    streams_of = jax.random.split(jax.random.key(seed), 18)
    tokens = draw_tokens(jax.random.fold_in(streams_of[17], 71), 0)
    norm_gain = jnp.clip(1.0 + 0.18 * jax.random.normal(streams_of[1], (LAYERS, D), jnp.float32), 0.1, 1.9)
    w_gate = noise(streams_of[2], (LAYERS, D, SSDW), D ** -0.5, 0.09375, ((2, 32),))
    w_value = noise(streams_of[3], (LAYERS, D, SSDW), D ** -0.5, 0.09375, ((2, 32),))
    w_write = noise(streams_of[4], (LAYERS, D, GROUPS * STATE), D ** -0.5, 0.09375, ((2, 32),))
    w_read = noise(streams_of[5], (LAYERS, D, GROUPS * STATE), D ** -0.5, 0.09375, ((2, 32),))
    w_step = noise(streams_of[6], (LAYERS, D, HEADS), D ** -0.5, 0.09375)
    step_bias = jnp.clip(jax.random.uniform(streams_of[7], (LAYERS, HEADS), jnp.float32, -2.0, 1.0), -2.0, 1.0)
    decay_rate = jnp.clip(jnp.exp(jax.random.uniform(streams_of[8], (LAYERS, HEADS), jnp.float32, math.log(0.05), math.log(3.0))), 0.05, 3.0)
    skip_gain = jnp.clip(jnp.exp(jax.random.uniform(streams_of[9], (LAYERS, HEADS), jnp.float32, math.log(1.0), math.log(4.0))), 1.0, 4.0)
    conv_value_weight = noise(streams_of[10], (LAYERS, CONV, SSDW), 0.577, 2.5, ((2, 32),), jnp.float32)
    conv_key_weight = noise(streams_of[11], (LAYERS, CONV, 2, GROUPS * STATE), 0.577, 2.5, ((3, 32),), jnp.float32)
    group_gain = jnp.clip(1.0 + 0.18 * jax.random.normal(streams_of[12], (LAYERS, SSDW), jnp.float32), 0.1, 1.9)
    w_out = noise(streams_of[13], (LAYERS, SSDW, D), SSDW ** -0.5, 0.0625, ((1, 32),))
    ssm_state = noise(streams_of[14], (LAYERS, BATCH, SSDW, STATE), 0.5, 3.0, ((2, 32),), jnp.float32)
    conv_value = noise(streams_of[15], (LAYERS, BATCH, CONV - 1, SSDW), 1.0, 5.0, ((3, 32),), jnp.float32)
    conv_key = noise(streams_of[16], (LAYERS, BATCH, CONV - 1, 2, GROUPS * STATE), 1.0, 5.0, ((4, 32),), jnp.float32)
    return {"tokens": tokens, "norm_gain": norm_gain, "w_gate": w_gate, "w_value": w_value, "w_write": w_write, "w_read": w_read, "w_step": w_step, "step_bias": step_bias, "decay_rate": decay_rate, "skip_gain": skip_gain, "conv_value_weight": conv_value_weight, "conv_key_weight": conv_key_weight, "group_gain": group_gain, "w_out": w_out, "ssm_state": ssm_state, "conv_value": conv_value, "conv_key": conv_key}


EPS = 1e-06

def reference(tokens, norm_gain, w_gate, w_value, w_write, w_read, w_step, step_bias, decay_rate, skip_gain, conv_value_weight, conv_key_weight, group_gain, w_out, ssm_state, conv_value, conv_key):
    hidden = tokens
    ssm_list = []
    value_list = []
    key_list = []
    for layer in range(LAYERS):
        resid = hidden.astype(jnp.float32)
        inv_scale = lax.rsqrt(lax.optimization_barrier(jnp.sum(resid * resid, axis=1)) / D + EPS)[:, None]
        scaled = (resid * norm_gain[layer]).astype(jnp.bfloat16)

        def project(weight):
            return jnp.dot(scaled, weight[layer], preferred_element_type=jnp.float32) * inv_scale
        gate_in = project(w_gate)
        value_in = project(w_value)
        write_in = project(w_write)
        read_in = project(w_read)
        step_in = project(w_step)
        value_window = jnp.concatenate([conv_value[layer], value_in[:, None, :]], axis=1)
        value_list.append(value_window[:, 1:])
        values = jax.nn.silu(lax.optimization_barrier(jnp.sum(value_window * conv_value_weight[layer][None], axis=1)))
        values = values.reshape(BATCH, GROUPS, HPG, HEAD_DIM)
        fresh = jnp.stack([write_in, read_in], axis=1)[:, None]
        key_window = jnp.concatenate([conv_key[layer], fresh], axis=1)
        key_list.append(key_window[:, 1:])
        mixed_keys = jax.nn.silu(lax.optimization_barrier(jnp.sum(key_window * conv_key_weight[layer][None], axis=1)))
        writes = jnp.transpose(mixed_keys[:, 0].reshape(BATCH, STATE, GROUPS), (0, 2, 1))
        reads = jnp.transpose(mixed_keys[:, 1].reshape(BATCH, STATE, GROUPS), (0, 2, 1))
        delta = jax.nn.softplus(step_in + step_bias[layer][None])
        decay = jnp.exp(-delta * decay_rate[layer][None])
        delta = delta.reshape(BATCH, GROUPS, HPG)
        decay = decay.reshape(BATCH, GROUPS, HPG)
        state = ssm_state[layer].reshape(BATCH, GROUPS, HPG, HEAD_DIM, STATE)
        state = decay[..., None, None] * state + (delta[..., None] * values)[..., None] * writes[:, :, None, None, :]
        ssm_list.append(state.reshape(BATCH, SSDW, STATE))
        read_out = jnp.einsum('bghpn,bgn->bghp', state, reads, precision=lax.Precision.HIGHEST)
        read_out = read_out + skip_gain[layer].reshape(GROUPS, HPG)[None, :, :, None] * values
        gated = read_out.reshape(BATCH, GROUPS, GW) * jax.nn.silu(gate_in.reshape(BATCH, GROUPS, GW))
        group_scale = lax.rsqrt(lax.optimization_barrier(jnp.mean(gated * gated, axis=2, keepdims=True)) + EPS)
        normed = (gated * group_scale * group_gain[layer].reshape(GROUPS, GW)[None]).astype(jnp.bfloat16)
        update = jnp.dot(normed.reshape(BATCH, SSDW), w_out[layer], preferred_element_type=jnp.float32)
        hidden = (resid + update).astype(jnp.bfloat16)
    return (hidden, jnp.stack(ssm_list), jnp.stack(value_list), jnp.stack(key_list))
```

```python
import jax
import jax.numpy as jnp
from jax import lax
from jax.experimental import pallas as pl
from jax.experimental.pallas import tpu as pltpu
from jax.sharding import PartitionSpec as P
import functools

D = 4096
HEAD_DIM = 64
GROUPS = 8
STATE = 128
LAYERS = 2
HEADS = 128
GW = 1024


EPS = 1e-06


def per_device(
    tokens,
    norm_gain,
    w_gate,
    w_value,
    w_write,
    w_read,
    w_step,
    step_bias,
    decay_rate,
    skip_gain,
    conv_value_weight,
    conv_key_weight,
    group_gain,
    w_out,
    ssm_state,
    conv_value,
    conv_key,
):
    highest = lax.Precision.HIGHEST
    chan_count = w_gate.shape[2]
    position = lax.axis_index("tp")
    first_chan = position * chan_count
    chan_ids = first_chan + jnp.arange(chan_count, dtype=jnp.int32)
    my_group = first_chan // GW
    head_hot = (
        (chan_ids // HEAD_DIM)[:, None] == jnp.arange(HEADS, dtype=jnp.int32)[None, :]
    ).astype(jnp.float32)
    group_hot = ((chan_ids // GW)[:, None] == jnp.arange(GROUPS, dtype=jnp.int32)[None, :]).astype(
        jnp.float32
    )
    hidden = tokens
    ssm_list = []
    value_list = []
    key_list = []
    for layer in range(LAYERS):
        resid = hidden.astype(jnp.float32)
        inv_scale = lax.rsqrt(jnp.sum(resid * resid, axis=1) / D + EPS)[:, None]
        scaled = (resid * norm_gain[layer]).astype(jnp.bfloat16)

        def project(weight):
            return jnp.dot(scaled, weight[layer], preferred_element_type=jnp.float32) * inv_scale

        gate_in = project(w_gate)
        value_in = project(w_value)
        write_in = project(w_write)
        read_in = project(w_read)
        step_in = project(w_step)
        value_window = jnp.concatenate([conv_value[layer], value_in[:, None, :]], axis=1)
        value_list.append(value_window[:, 1:])
        values = jax.nn.silu(jnp.sum(value_window * conv_value_weight[layer][None], axis=1))
        fresh = jnp.stack([write_in, read_in], axis=1)[:, None]
        key_window = jnp.concatenate([conv_key[layer], fresh], axis=1)
        key_list.append(key_window[:, 1:])
        mixed_keys = jax.nn.silu(jnp.sum(key_window * conv_key_weight[layer][None], axis=1))
        every_group = lax.all_gather(mixed_keys, "tp", axis=2, tiled=True)
        by_entry = every_group.reshape(every_group.shape[0], 2, STATE, GROUPS)
        own_keys = lax.dynamic_slice_in_dim(by_entry, my_group, 1, 3)[..., 0]
        writes = own_keys[:, 0]
        reads = own_keys[:, 1]
        delta = jax.nn.softplus(step_in + step_bias[layer][None])
        decay = jnp.exp(-delta * decay_rate[layer][None])
        delta_chan = jnp.dot(delta, head_hot.T, precision=highest)
        decay_chan = jnp.dot(decay, head_hot.T, precision=highest)
        skip_chan = jnp.dot(skip_gain[layer], head_hot.T, precision=highest)
        state = (
            decay_chan[..., None] * ssm_state[layer]
            + (delta_chan * values)[..., None] * writes[:, None, :]
        )
        ssm_list.append(state)
        read_out = jnp.sum(state * reads[:, None, :], axis=2) + skip_chan[None] * values
        gated = read_out * jax.nn.silu(gate_in)
        squares = jnp.dot(gated * gated, group_hot, precision=highest)
        square_total = lax.psum(squares, "tp")
        group_scale = lax.rsqrt(square_total / GW + EPS)
        scale_chan = jnp.dot(group_scale, group_hot.T, precision=highest)
        normed = (gated * scale_chan * group_gain[layer][None]).astype(jnp.bfloat16)
        partial_out = jnp.dot(normed, w_out[layer], preferred_element_type=jnp.float32)
        update = lax.psum(partial_out, "tp")
        hidden = (resid + update).astype(jnp.bfloat16)
    return (hidden, jnp.stack(ssm_list), jnp.stack(value_list), jnp.stack(key_list))


LANES = 128
TAPS = 3
VMEM = 67043328
BF16 = jnp.bfloat16
F32 = jnp.float32
NT = (((1,), (1,)), ((), ()))


def split3(x):
    high = x.astype(BF16)
    rest = x - high.astype(F32)
    mid = rest.astype(BF16)
    return high, mid, (rest - mid.astype(F32)).astype(BF16)


def select_dot(x, hot):
    rows = x.shape[0]
    parts = jnp.concatenate(split3(x), axis=0)
    out = jnp.dot(parts, hot, preferred_element_type=F32)
    return out[:rows] + out[rows : 2 * rows] + out[2 * rows :]


def silu(v):
    return v / (1.0 + jnp.exp(-v))


def iota(shape, axis):
    return lax.broadcasted_iota(jnp.int32, shape, axis)


def mixer(
    n,
    tokens_hbm,
    gain_hbm,
    wg_hbm,
    wv_hbm,
    ww_hbm,
    wr_hbm,
    ws_hbm,
    bias_hbm,
    rate_hbm,
    skip_hbm,
    cvw_hbm,
    ckw_hbm,
    gg_hbm,
    wo_hbm,
    state_hbm,
    cv_hbm,
    ck_hbm,
    tokens_out,
    state,
    value_out,
    key_out,
    tokens,
    gain,
    wg,
    wv,
    wk,
    ws,
    bias,
    rate,
    skip,
    cvw,
    ckw,
    gg,
    wo,
    cv,
    ck,
    hidden,
    scaled,
    keys_send,
    keys_recv,
    pair_send,
    pair_recv,
    part,
    rs_send,
    rs_recv,
    sq_own,
    sq_pair,
    sq_send,
    sq_recv,
    scales,
    turned,
    cols,
    wbuf,
    in_small,
    in_big,
    key_ss,
    key_rs,
    pair_ss,
    pair_rs,
    sp_ss,
    sp_rs,
    sq_ss,
    sq_rs,
    rs_ss,
    rs_rs,
    ag_ss,
    ag_rs,
    fw_ss,
    fw_rs,
):
    layers, batch, chans, entries = state.shape
    depth = tokens.shape[1]
    chips = n // 2
    block = depth // chips
    key_cols = wk.shape[1] // 2
    own_entries = key_cols // GROUPS
    heads = bias.shape[1]
    peers = GW // chans
    per_group = peers // 2
    me = lax.axis_index("tp")
    chip = me // 2
    core = lax.rem(me, 2)
    other = 1 - core
    buddy = 2 * chip + other
    my_group = me // peers

    small_pairs = (
        (tokens_hbm, tokens),
        (gain_hbm, gain),
        (ck_hbm, ck),
        (ckw_hbm, ckw),
        (bias_hbm, bias),
        (rate_hbm, rate),
        (skip_hbm, skip),
        (cvw_hbm, cvw),
        (gg_hbm, gg),
        (cv_hbm, cv),
    )
    small = [pltpu.make_async_copy(a, b, in_small.at[i]) for i, (a, b) in enumerate(small_pairs)]
    big = [
        [
            pltpu.make_async_copy(a.at[l], b.at[l], in_big.at[l, i])
            for i, (a, b) in enumerate(
                (
                    (ww_hbm, wk.at[:, :key_cols]),
                    (wr_hbm, wk.at[:, key_cols:]),
                    (wg_hbm, wg),
                    (wv_hbm, wv),
                    (ws_hbm, ws),
                    (state_hbm, state),
                    (wo_hbm, wo),
                )
            )
        ]
        for l in range(layers)
    ]
    for copy in small[:4] + big[0][:2]:
        copy.start()

    def flipped(value, mask):
        bit = 1
        out = value
        while bit <= mask:
            if mask & bit:
                out = out + bit - 2 * bit * lax.rem(value // bit, 2)
            bit *= 2
        return out

    chip_of = [flipped(chip, m) for m in range(chips)]

    def distance(m):
        return (m >> 2) + (m >> 1) % 2 + m % 2

    near = sorted(range(chips), key=lambda m: (distance(m), m))
    far = near[::-1]

    barrier = pltpu.get_barrier_semaphore()

    def signal(to):
        pl.semaphore_signal(barrier, inc=1, device_id=(to,), device_id_type=pl.DeviceIdType.MESH)

    for m in far[:-1]:
        signal(2 * chip_of[m])
        signal(2 * chip_of[m] + 1)
    signal(buddy)

    def remote(src, dst, ss, rs, to):
        return pltpu.make_async_remote_copy(
            src_ref=src,
            dst_ref=dst,
            send_sem=ss,
            recv_sem=rs,
            device_id=(to,),
            device_id_type=pl.DeviceIdType.MESH,
        )

    row = iota((2 * LANES, 2 * entries), 0)
    col = iota((2 * LANES, 2 * entries), 1)
    half = row // LANES
    inner = row % LANES
    entry = half * 2 + inner // (LANES // 2)
    sender = (inner % (LANES // 2)) // 2
    recv_hot = jnp.where(
        col == (inner % 2) * entries + sender * own_entries + entry, 1.0, 0.0
    ).astype(BF16)
    row = iota((heads, chans), 0)
    col = iota((heads, chans), 1)
    head_hot = jnp.where(row == (me * chans + col) // HEAD_DIM, 1.0, 0.0).astype(BF16)

    groups8 = batch // 8

    def update_state(l, group):
        shifted = pltpu.roll(cols[...], lax.rem(LANES - 8 * group, LANES), 1)
        writes8 = wbuf[pl.ds(pl.multiple_of(8 * group, 8), 8), :]
        for j in range(8):
            b = 8 * group + j
            state[l, b] = (
                shifted[:, batch + j : batch + j + 1] * state[l, b]
                + shifted[:, j : j + 1] * writes8[j : j + 1, :]
            )

    def update_range(l, low, high):
        def step(g, carry):
            update_state(l, g)
            return carry

        lax.fori_loop(low, high, step, 0)

    def at_chip(c):
        return pl.ds(pl.multiple_of(c * block, block), block)

    def prepare(l, pos, c, squares):
        if l == 0:
            x = tokens[:, at_chip(c)].astype(F32)
        else:
            x = jnp.concatenate([hidden[l - 1, 2 * c], hidden[l - 1, 2 * c + 1]], axis=1).astype(F32)
        scaled[pos] = (x * gain[l : l + 1, at_chip(c)]).astype(BF16)
        return squares + x * x

    def key_dot(l, pos, c, acc):
        return acc + lax.dot_general(
            scaled[pos], wk[l, :, at_chip(c)], NT, preferred_element_type=F32
        )

    def main_dots(l, pos, c, accs):
        return tuple(
            acc + jnp.dot(scaled[pos], ref[l, at_chip(c), :], preferred_element_type=F32)
            for acc, ref in zip(accs, (wg, wv, ws))
        )

    def send_keys(l, key_acc, squares):
        inv_scale = lax.rsqrt(jnp.sum(squares, axis=1, keepdims=True) / depth + EPS)
        key_in = key_acc * inv_scale
        mixed = []
        for i in range(2):
            fresh = key_in[:, i * key_cols : (i + 1) * key_cols]
            total = fresh * ckw[l, TAPS - 1, i : i + 1, :]
            for k in range(TAPS - 1):
                total = total + ck[l, :, k, i, :] * ckw[l, k, i : i + 1, :]
            mixed.append(silu(total))
        mixed = jnp.concatenate(
            mixed + [jnp.zeros((batch, LANES - 2 * key_cols), F32)], axis=1
        )
        spread = jnp.concatenate([mixed] * own_entries, axis=0).T
        lane_entry = iota((GROUPS, LANES), 1) // batch
        for i in range(2):
            packed = jnp.zeros((GROUPS, LANES), F32)
            for e in range(own_entries):
                at = (i * own_entries + e) * GROUPS
                packed = jnp.where(lane_entry == e, spread[at : at + GROUPS], packed)
            keys_send[l, :, i, :] = packed
        keys_recv[l, me] = keys_send[l, my_group]
        if l == 0:
            pl.semaphore_wait(barrier, n - 1)
        for m in far:
            for to in ([2 * chip_of[m], 2 * chip_of[m] + 1] if m else [buddy]):
                remote(
                    keys_send.at[l, to // peers], keys_recv.at[l, me], key_ss.at[l], key_rs.at[l], to
                ).start()
        return inv_scale, key_in

    zeros = tuple(jnp.zeros((batch, ref.shape[2]), F32) for ref in (wg, wv, ws))
    key_zero = jnp.zeros((batch, 2 * key_cols), F32)
    square_zero = jnp.zeros((batch, block), F32)

    def ag_wait(l, m):
        return remote(
            hidden.at[l, 2 * chip_of[m] + other], hidden.at[l, 2 * chip_of[m] + other],
            ag_ss.at[l], ag_rs.at[l, m], buddy,
        )

    def forward(l, m):
        s = 2 * chip_of[m] + other
        return remote(hidden.at[l, s], hidden.at[l, s], fw_ss.at[l], fw_rs.at[l, m], buddy)

    def forward_all(l, masks):
        for m in masks:
            if m:
                ag_wait(l, m).wait_recv()
                forward(l, m).start()

    def whole(l, masks):
        for m in masks:
            if m:
                forward(l, m).wait_recv()
            else:
                ag_wait(l, 0).wait_recv()

    for l in range(layers):
        if l == 0:
            for copy in small[:4] + big[0][:2]:
                copy.wait()
            for copy in big[0][2:5] + small[4:]:
                copy.start()
            squares = square_zero
            key_acc = key_zero
            for c in range(chips):
                squares = prepare(l, c, c, squares)
                key_acc = key_dot(l, c, c, key_acc)
            inv_scale, key_in = send_keys(l, key_acc, squares)
            for copy in big[0][2:5]:
                copy.wait()
            for copy in big[0][5:]:
                copy.start()
            accs = zeros
            for c in range(chips):
                accs = main_dots(l, c, c, accs)
            for copy in small[4:]:
                copy.wait()
        else:
            for copy in big[l][:5]:
                copy.wait()
            quarter = chips // 4
            squares, key_acc, accs = square_zero, key_zero, zeros
            waves = [near[q * quarter : (q + 1) * quarter] for q in range(4)]
            forward_all(l - 1, waves[0])
            forward_all(l - 1, waves[1])
            for q, wave in enumerate(waves):
                whole(l - 1, wave)
                for i, m in enumerate(wave):
                    pos = q * quarter + i
                    squares = prepare(l, pos, chip_of[m], squares)
                    key_acc = key_dot(l, pos, chip_of[m], key_acc)
                if q < 3:
                    for i, m in enumerate(wave):
                        accs = main_dots(l, q * quarter + i, chip_of[m], accs)
                if q < 2:
                    forward_all(l - 1, waves[q + 2])
            inv_scale, key_in = send_keys(l, key_acc, squares)
            for i, m in enumerate(waves[3]):
                accs = main_dots(l, 3 * quarter + i, chip_of[m], accs)
        gate_in, value_in, step_in = [acc * inv_scale for acc in accs]
        for i in range(2):
            for k in range(1, TAPS - 1):
                key_out[l, :, k - 1, i, :] = ck[l, :, k, i, :]
            key_out[l, :, TAPS - 2, i, :] = key_in[:, i * key_cols : (i + 1) * key_cols]
        for k in range(1, TAPS - 1):
            value_out[l, :, k - 1, :] = cv[l, :, k, :]
        value_out[l, :, TAPS - 2, :] = value_in
        values = value_in * cvw[TAPS - 1, l : l + 1, :]
        for k in range(TAPS - 1):
            values = values + cv[l, :, k, :] * cvw[k, l : l + 1, :]
        values = silu(values)
        raw = step_in + bias[l : l + 1, :]
        delta = jnp.maximum(raw, 0.0) + jnp.log1p(jnp.exp(-jnp.abs(raw)))
        decay = jnp.exp(-delta * rate[l : l + 1, :])
        skips = jnp.broadcast_to(skip[l : l + 1, :], (8, heads))
        chan = select_dot(jnp.concatenate([delta, decay, skips], axis=0), head_hot)
        decay_chan = chan[batch : 2 * batch]
        skip_chan = chan[2 * batch : 2 * batch + 1]
        dv = chan[:batch] * values
        cols[...] = jnp.concatenate(
            [dv, decay_chan, jnp.zeros((LANES - 2 * batch, chans), F32)], axis=0
        ).T
        gate = silu(gate_in)
        big[l][5].wait()

        def turn(g, carry):
            for j in range(4):
                turned[4 * g + j] = state[l, 4 * g + j].T.astype(BF16)
            return carry

        lax.fori_loop(0, batch // 4, turn, 0)
        big[l][6].wait()

        remote(
            keys_recv.at[l, pl.ds(0, n - 1)], keys_recv.at[l, pl.ds(0, n - 1)],
            key_ss.at[l], key_rs.at[l], buddy,
        ).wait_recv()
        arrived = keys_recv[l].reshape(2 * n, LANES)
        arrived = jnp.concatenate([arrived, arrived], axis=0).T
        left_half = iota((batch, LANES), 1) < LANES // 2
        pieces = [
            jnp.where(
                left_half,
                arrived[2 * h * batch : (2 * h + 1) * batch],
                arrived[(2 * h + 1) * batch : (2 * h + 2) * batch],
            )
            for h in range(2)
        ]
        both = select_dot(jnp.concatenate(pieces, axis=1), recv_hot)
        writes = both[:, :entries]
        reads = both[:, entries:]
        wbuf[...] = writes
        lane_half = iota((8, 2 * entries), 1) // entries
        sub = iota((8, 2 * entries), 0)
        query = []
        for g in range(groups8):
            reads8 = reads[8 * g : 8 * g + 8]
            twice = jnp.concatenate([reads8, reads8], axis=1)
            total = jnp.zeros((8, chans), F32)
            for p in range(4):
                left = jnp.where(sub == 2 * p + lane_half, twice, 0.0).astype(BF16)
                right = turned[pl.ds(8 * g + 2 * p, 2)].reshape(2 * entries, chans)
                total = total + jnp.dot(left, right, preferred_element_type=F32)
            query.append(total)
        query = jnp.concatenate(query, axis=0)
        through = jnp.sum(writes * reads, axis=1, keepdims=True)
        mixed_out = decay_chan * query + dv * through + skip_chan * values
        gated = mixed_out * gate
        fed = (gated * gg[l : l + 1, :]).astype(BF16)

        def out_pair(i, parity):
            rhs = jnp.concatenate(
                [
                    wo[l, :, pl.ds(pl.multiple_of((2 * chip_of[far[i + j]] + parity) * LANES, LANES), LANES)]
                    for j in range(2)
                ],
                axis=1,
            )
            return jnp.dot(fed, rhs, preferred_element_type=F32)

        quarter = chips // 4

        def pair_copy(q):
            at = pl.ds(q * quarter, quarter)
            return remote(
                pair_send.at[l, at], pair_recv.at[l, at], pair_ss.at[l, q], pair_rs.at[l, q], buddy
            )

        for q in range(4):
            for i in range(q * quarter, (q + 1) * quarter, 2):
                res = out_pair(i, core).astype(BF16)
                pair_send[l, i] = res[:, :LANES]
                pair_send[l, i + 1] = res[:, LANES:]
            pair_copy(q).start()
        square = gated * gated
        square = square[:, :LANES] + square[:, LANES:]
        square = jnp.concatenate([square, jnp.zeros((LANES - batch, LANES), F32)], axis=0).T
        sq_own[l] = jnp.sum(square, axis=0, keepdims=True)
        sp_copy = remote(sq_own.at[l], sq_pair.at[l], sp_ss.at[l], sp_rs.at[l], buddy)
        sp_copy.start()
        for i in range(0, chips, 2):
            res = out_pair(i, other)
            part[i] = res[:, :LANES]
            part[i + 1] = res[:, LANES:]

        def rs_copy(i):
            return remote(
                rs_send.at[l, i], rs_recv.at[l, chip], rs_ss.at[l], rs_rs.at[l], 2 * chip_of[far[i]] + other
            )

        for q in range(4):
            pair_copy(q).wait_recv()
            for i in range(q * quarter, (q + 1) * quarter):
                rs_send[l, i] = (part[i] + pair_recv[l, i].astype(F32)).astype(BF16)
                rs_copy(i).start()
        sp_copy.wait_recv()
        sq_send[l] = sq_own[l] + sq_pair[l]
        for m in far:
            remote(
                sq_send.at[l], sq_recv.at[l, chip], sq_ss.at[l], sq_rs.at[l], 2 * chip_of[m] + other
            ).start()
        if l + 1 < layers:
            for copy in big[l + 1]:
                copy.start()
        update_range(l, 0, groups8)
        remote(sq_recv.at[l], sq_recv.at[l], sq_ss.at[l], sq_rs.at[l], buddy).wait_recv()
        rows = []
        for g in range(GROUPS):
            total = sq_recv[l, per_group * g]
            for k in range(1, per_group):
                total = total + sq_recv[l, per_group * g + k]
            rows.append(total)
        rows = lax.rsqrt(jnp.concatenate(rows, axis=0) / GW + EPS)
        columns = jnp.concatenate([rows, jnp.zeros((LANES - GROUPS, LANES), F32)], axis=0).T
        for g in range(GROUPS):
            scales[g] = jnp.broadcast_to(columns[:batch, g : g + 1], (batch, LANES))
        if l == 0:
            resid = tokens[:, pl.ds(pl.multiple_of(me * LANES, LANES), LANES)]
        else:
            resid = hidden[l - 1, me]
        remote(rs_recv.at[l], rs_recv.at[l], rs_ss.at[l], rs_rs.at[l], buddy).wait_recv()
        sums = [resid.astype(F32)] + [jnp.zeros((batch, LANES), F32)] * 3
        for g in range(GROUPS):
            term = rs_recv[l, per_group * g].astype(F32)
            for k in range(1, per_group):
                term = term + rs_recv[l, per_group * g + k].astype(F32)
            sums[g % 4] = sums[g % 4] + term * scales[g]
        hidden[l, me] = ((sums[0] + sums[1]) + (sums[2] + sums[3])).astype(BF16)
        for m in far:
            remote(
                hidden.at[l, me], hidden.at[l, me], ag_ss.at[l], ag_rs.at[l, m], 2 * chip_of[m] + other
            ).start()

    forward_all(layers - 1, near)
    whole(layers - 1, near)
    for j in range(n):
        tokens_out[:, j * LANES : (j + 1) * LANES] = hidden[layers - 1, j]
    for l in range(layers):
        def sent(src, sem):
            remote(src, src, sem, rs_rs.at[l], buddy).wait_send()

        sent(keys_recv.at[l, pl.ds(0, n - 1)], key_ss.at[l])
        for q in range(4):
            sent(pair_send.at[l, pl.ds(0, chips // 4)], pair_ss.at[l, q])
        sent(sq_own.at[l], sp_ss.at[l])
        sent(sq_recv.at[l], sq_ss.at[l])
        sent(rs_send.at[l], rs_ss.at[l])
        sent(hidden.at[l, pl.ds(0, chips)], ag_ss.at[l])
        sent(hidden.at[l, pl.ds(0, chips - 1)], fw_ss.at[l])


def flush(tokens, state, value, key, tokens_hbm, state_hbm, value_hbm, key_hbm, sems):
    layers, batch = state.shape[:2]
    step = batch // 4
    copies = [
        pltpu.make_async_copy(key, key_hbm, sems.at[0]),
        pltpu.make_async_copy(value, value_hbm, sems.at[1]),
        pltpu.make_async_copy(tokens, tokens_hbm, sems.at[2]),
    ]
    for l in range(layers):
        for i in range(4):
            at = pl.ds(i * step, step)
            copies.append(
                pltpu.make_async_copy(state.at[l, at], state_hbm.at[l, at], sems.at[len(copies)])
            )
    for copy in copies:
        copy.start()
    for copy in copies:
        copy.wait()


def fused(n, *args):
    (tokens, norm_gain, w_gate, w_value, w_write, w_read, w_step, step_bias, decay_rate) = args[:9]
    (skip_gain, cvw, ckw, group_gain, w_out, ssm_state, conv_value, conv_key) = args[9:]
    layers, batch, chans, entries = ssm_state.shape
    depth = tokens.shape[1]
    chips = n // 2
    key_cols = w_write.shape[2]
    operands = list(args)
    operands[4] = jnp.swapaxes(w_write, 1, 2)
    operands[5] = jnp.swapaxes(w_read, 1, 2)
    operands[10] = jnp.swapaxes(cvw, 0, 1)
    landed = [pltpu.VMEM(a.shape, a.dtype) for a in operands]
    landed[4:6] = [pltpu.VMEM((layers, 2 * key_cols, depth), BF16)]
    del landed[13]
    dma = pltpu.SemaphoreType.DMA
    outs = (
        jax.ShapeDtypeStruct(tokens.shape, BF16),
        jax.ShapeDtypeStruct(ssm_state.shape, F32),
        jax.ShapeDtypeStruct(conv_value.shape, F32),
        jax.ShapeDtypeStruct(conv_key.shape, F32),
    )
    small_bytes = 4 * 1024 * 1024
    results = pl.pallas_call(
        functools.partial(mixer, n),
        out_shape=tuple(pltpu.VMEM(o.shape, o.dtype) for o in outs),
        in_specs=[pl.BlockSpec(memory_space=pltpu.HBM)] * len(operands),
        out_specs=(pl.BlockSpec(memory_space=pltpu.VMEM),) * 4,
        scratch_shapes=landed
        + [
            pltpu.VMEM((layers, n, batch, LANES), BF16),
            pltpu.VMEM((chips, batch, depth // chips), BF16),
            pltpu.VMEM((layers, GROUPS, 2, LANES), F32),
            pltpu.VMEM((layers, n, 2, LANES), F32),
            pltpu.VMEM((layers, chips, batch, LANES), BF16),
            pltpu.VMEM((layers, chips, batch, LANES), BF16),
            pltpu.VMEM((chips, batch, LANES), F32),
            pltpu.VMEM((layers, chips, batch, LANES), BF16),
            pltpu.VMEM((layers, chips, batch, LANES), BF16),
            pltpu.VMEM((layers, 1, LANES), F32),
            pltpu.VMEM((layers, 1, LANES), F32),
            pltpu.VMEM((layers, 1, LANES), F32),
            pltpu.VMEM((layers, chips, 1, LANES), F32),
            pltpu.VMEM((GROUPS, batch, LANES), F32),
            pltpu.VMEM((batch, entries, chans), BF16),
            pltpu.VMEM((chans, LANES), F32),
            pltpu.VMEM((batch, entries), F32),
            dma((10,)),
            dma((layers, 7)),
            dma((layers,)),
            dma((layers,)),
            dma((layers, 4)),
            dma((layers, 4)),
            dma((layers,)),
            dma((layers,)),
            dma((layers,)),
            dma((layers,)),
            dma((layers,)),
            dma((layers,)),
            dma((layers,)),
            dma((layers, chips)),
            dma((layers,)),
            dma((layers, chips)),
        ],
        compiler_params=pltpu.CompilerParams(
            collective_id=0,
            has_side_effects=True,
            vmem_limit_bytes=VMEM - ssm_state.size * 4 - small_bytes,
        ),
        name="mixer",
    )(*operands)
    return pl.pallas_call(
        flush,
        out_shape=outs,
        in_specs=[pl.BlockSpec(memory_space=pl.ANY)] * 4,
        out_specs=(pl.BlockSpec(memory_space=pltpu.HBM),) * 4,
        scratch_shapes=[dma((3 + 4 * layers,))],
        compiler_params=pltpu.CompilerParams(vmem_limit_bytes=1024 * 1024),
        name="flush",
    )(*results)


def dispatch(n, *args):
    depth = args[0].shape[1]
    layers, batch, chans, entries = args[14].shape
    own_entries = args[4].shape[2] // GROUPS
    fits = (
        depth == n * LANES
        and n == 32
        and own_entries == 4
        and own_entries * batch == LANES
        and entries == LANES
        and chans == 2 * LANES
        and args[7].shape[1] == LANES
    )
    return fused(n, *args) if fits else per_device(*args)


def solution(mesh):
    placed = (
        P(),
        P(),
        P(None, None, "tp"),
        P(None, None, "tp"),
        P(None, None, "tp"),
        P(None, None, "tp"),
        P(),
        P(),
        P(),
        P(),
        P(None, None, "tp"),
        P(None, None, None, "tp"),
        P(None, "tp"),
        P(None, "tp", None),
        P(None, None, "tp", None),
        P(None, None, None, "tp"),
        P(None, None, None, None, "tp"),
    )
    return jax.shard_map(
        functools.partial(dispatch, mesh.shape["tp"]),
        mesh=mesh,
        in_specs=placed,
        out_specs=(
            P(),
            P(None, None, "tp", None),
            P(None, None, None, "tp"),
            P(None, None, None, None, "tp"),
        ),
        check_vma=False,
    )
```

```python
import jax
import jax.numpy as jnp
from jax import lax
from jax.experimental import pallas as pl
from jax.experimental.pallas import tpu as pltpu
from jax.sharding import PartitionSpec as P
import functools

D = 4096
HEAD_DIM = 64
GROUPS = 8
STATE = 128
LAYERS = 2
HEADS = 128
GW = 1024


EPS = 1e-06


def per_device(
    tokens,
    norm_gain,
    w_gate,
    w_value,
    w_write,
    w_read,
    w_step,
    step_bias,
    decay_rate,
    skip_gain,
    conv_value_weight,
    conv_key_weight,
    group_gain,
    w_out,
    ssm_state,
    conv_value,
    conv_key,
):
    highest = lax.Precision.HIGHEST
    chan_count = w_gate.shape[2]
    position = lax.axis_index("tp")
    first_chan = position * chan_count
    chan_ids = first_chan + jnp.arange(chan_count, dtype=jnp.int32)
    my_group = first_chan // GW
    head_hot = (
        (chan_ids // HEAD_DIM)[:, None] == jnp.arange(HEADS, dtype=jnp.int32)[None, :]
    ).astype(jnp.float32)
    group_hot = ((chan_ids // GW)[:, None] == jnp.arange(GROUPS, dtype=jnp.int32)[None, :]).astype(
        jnp.float32
    )
    hidden = tokens
    ssm_list = []
    value_list = []
    key_list = []
    for layer in range(LAYERS):
        resid = hidden.astype(jnp.float32)
        inv_scale = lax.rsqrt(jnp.sum(resid * resid, axis=1) / D + EPS)[:, None]
        scaled = (resid * norm_gain[layer]).astype(jnp.bfloat16)

        def project(weight):
            return jnp.dot(scaled, weight[layer], preferred_element_type=jnp.float32) * inv_scale

        gate_in = project(w_gate)
        value_in = project(w_value)
        write_in = project(w_write)
        read_in = project(w_read)
        step_in = project(w_step)
        value_window = jnp.concatenate([conv_value[layer], value_in[:, None, :]], axis=1)
        value_list.append(value_window[:, 1:])
        values = jax.nn.silu(jnp.sum(value_window * conv_value_weight[layer][None], axis=1))
        fresh = jnp.stack([write_in, read_in], axis=1)[:, None]
        key_window = jnp.concatenate([conv_key[layer], fresh], axis=1)
        key_list.append(key_window[:, 1:])
        mixed_keys = jax.nn.silu(jnp.sum(key_window * conv_key_weight[layer][None], axis=1))
        every_group = lax.all_gather(mixed_keys, "tp", axis=2, tiled=True)
        by_entry = every_group.reshape(every_group.shape[0], 2, STATE, GROUPS)
        own_keys = lax.dynamic_slice_in_dim(by_entry, my_group, 1, 3)[..., 0]
        writes = own_keys[:, 0]
        reads = own_keys[:, 1]
        delta = jax.nn.softplus(step_in + step_bias[layer][None])
        decay = jnp.exp(-delta * decay_rate[layer][None])
        delta_chan = jnp.dot(delta, head_hot.T, precision=highest)
        decay_chan = jnp.dot(decay, head_hot.T, precision=highest)
        skip_chan = jnp.dot(skip_gain[layer], head_hot.T, precision=highest)
        state = (
            decay_chan[..., None] * ssm_state[layer]
            + (delta_chan * values)[..., None] * writes[:, None, :]
        )
        ssm_list.append(state)
        read_out = jnp.sum(state * reads[:, None, :], axis=2) + skip_chan[None] * values
        gated = read_out * jax.nn.silu(gate_in)
        squares = jnp.dot(gated * gated, group_hot, precision=highest)
        square_total = lax.psum(squares, "tp")
        group_scale = lax.rsqrt(square_total / GW + EPS)
        scale_chan = jnp.dot(group_scale, group_hot.T, precision=highest)
        normed = (gated * scale_chan * group_gain[layer][None]).astype(jnp.bfloat16)
        partial_out = jnp.dot(normed, w_out[layer], preferred_element_type=jnp.float32)
        update = lax.psum(partial_out, "tp")
        hidden = (resid + update).astype(jnp.bfloat16)
    return (hidden, jnp.stack(ssm_list), jnp.stack(value_list), jnp.stack(key_list))


LANES = 128
TAPS = 3
VMEM = 67043328
BF16 = jnp.bfloat16
F32 = jnp.float32
NT = (((1,), (1,)), ((), ()))


def split3(x):
    high = x.astype(BF16)
    rest = x - high.astype(F32)
    mid = rest.astype(BF16)
    return high, mid, (rest - mid.astype(F32)).astype(BF16)


def select_dot(x, hot):
    rows = x.shape[0]
    parts = jnp.concatenate(split3(x), axis=0)
    out = jnp.dot(parts, hot, preferred_element_type=F32)
    return out[:rows] + out[rows : 2 * rows] + out[2 * rows :]


def silu(v):
    return v / (1.0 + jnp.exp(-v))


def iota(shape, axis):
    return lax.broadcasted_iota(jnp.int32, shape, axis)


def mixer(
    n,
    tokens_hbm,
    gain_hbm,
    wg_hbm,
    wv_hbm,
    ww_hbm,
    wr_hbm,
    ws_hbm,
    bias_hbm,
    rate_hbm,
    skip_hbm,
    cvw_hbm,
    ckw_hbm,
    gg_hbm,
    wo_hbm,
    state_hbm,
    cv_hbm,
    ck_hbm,
    tokens_out,
    state,
    value_out,
    key_out,
    tokens,
    gain,
    wg,
    wv,
    wk,
    ws,
    bias,
    rate,
    skip,
    cvw,
    ckw,
    gg,
    wo,
    cv,
    ck,
    hidden,
    scaled,
    keys_send,
    keys_recv,
    pair_send,
    pair_recv,
    part,
    rs_send,
    rs_recv,
    sq_own,
    sq_pair,
    sq_send,
    sq_recv,
    scales,
    turned,
    cols,
    wbuf,
    in_sem,
    send_sem,
    recv_sem,
    pair_rs,
    ag_rs,
    fw_rs,
):
    key_ss, pair_ss, rs_ss, ag_ss, fw_ss, sp_ss, sq_ss = [send_sem.at[i] for i in range(7)]
    key_rs, sp_rs, sq_rs, rs_rs = [recv_sem.at[i] for i in range(4)]
    layers, batch, chans, entries = state.shape
    depth = tokens.shape[1]
    chips = n // 2
    block = depth // chips
    key_cols = wk.shape[1] // 2
    own_entries = key_cols // GROUPS
    heads = bias.shape[1]
    peers = GW // chans
    per_group = peers // 2
    me = lax.axis_index("tp")
    chip = me // 2
    core = lax.rem(me, 2)
    other = 1 - core
    buddy = 2 * chip + other
    my_group = me // peers

    small_pairs = (
        (tokens_hbm, tokens),
        (gain_hbm, gain),
        (ck_hbm, ck),
        (ckw_hbm, ckw),
        (bias_hbm, bias),
        (rate_hbm, rate),
        (skip_hbm, skip),
        (cvw_hbm, cvw),
        (gg_hbm, gg),
        (cv_hbm, cv),
    )
    small = [pltpu.make_async_copy(a, b, in_sem.at[i]) for i, (a, b) in enumerate(small_pairs)]
    big = [
        [
            pltpu.make_async_copy(a.at[l], b.at[l], in_sem.at[len(small_pairs) + i])
            for i, (a, b) in enumerate(
                (
                    (ww_hbm, wk.at[:, :key_cols]),
                    (wr_hbm, wk.at[:, key_cols:]),
                    (wg_hbm, wg),
                    (wv_hbm, wv),
                    (ws_hbm, ws),
                    (state_hbm, state),
                    (wo_hbm, wo),
                )
            )
        ]
        for l in range(layers)
    ]
    for copy in small[:4] + big[0][:2]:
        copy.start()

    def flipped(value, mask):
        bit = 1
        out = value
        while bit <= mask:
            if mask & bit:
                out = out + bit - 2 * bit * lax.rem(value // bit, 2)
            bit *= 2
        return out

    chip_of = [flipped(chip, m) for m in range(chips)]

    def distance(m):
        return (m >> 2) + (m >> 1) % 2 + m % 2

    near = sorted(range(chips), key=lambda m: (distance(m), m))
    far = near[::-1]

    barrier = pltpu.get_barrier_semaphore()

    def signal(to):
        pl.semaphore_signal(barrier, inc=1, device_id=(to,), device_id_type=pl.DeviceIdType.MESH)

    for m in far[:-1]:
        signal(2 * chip_of[m])
        signal(2 * chip_of[m] + 1)
    signal(buddy)

    def remote(src, dst, ss, rs, to):
        return pltpu.make_async_remote_copy(
            src_ref=src,
            dst_ref=dst,
            send_sem=ss,
            recv_sem=rs,
            device_id=(to,),
            device_id_type=pl.DeviceIdType.MESH,
        )

    row = iota((2 * LANES, 2 * entries), 0)
    col = iota((2 * LANES, 2 * entries), 1)
    half = row // LANES
    inner = row % LANES
    entry = half * 2 + inner // (LANES // 2)
    sender = (inner % (LANES // 2)) // 2
    recv_hot = jnp.where(
        col == (inner % 2) * entries + sender * own_entries + entry, 1.0, 0.0
    ).astype(BF16)
    row = iota((heads, chans), 0)
    col = iota((heads, chans), 1)
    head_hot = jnp.where(row == (me * chans + col) // HEAD_DIM, 1.0, 0.0).astype(BF16)

    groups8 = batch // 8

    def update_state(l, group):
        shifted = pltpu.roll(cols[...], lax.rem(LANES - 8 * group, LANES), 1)
        writes8 = wbuf[pl.ds(pl.multiple_of(8 * group, 8), 8), :]
        for j in range(8):
            b = 8 * group + j
            state[l, b] = (
                shifted[:, batch + j : batch + j + 1] * state[l, b]
                + shifted[:, j : j + 1] * writes8[j : j + 1, :]
            )

    def update_range(l, low, high):
        def step(g, carry):
            update_state(l, g)
            return carry

        lax.fori_loop(low, high, step, 0)

    def at_chip(c):
        return pl.ds(pl.multiple_of(c * block, block), block)

    def prepare(l, pos, c, squares):
        if l == 0:
            x = tokens[:, at_chip(c)].astype(F32)
        else:
            x = jnp.concatenate([hidden[l - 1, 2 * c], hidden[l - 1, 2 * c + 1]], axis=1).astype(F32)
        scaled[pos] = (x * gain[l : l + 1, at_chip(c)]).astype(BF16)
        return squares + x * x

    def key_dot(l, pos, c, acc):
        return acc + lax.dot_general(
            scaled[pos], wk[l, :, at_chip(c)], NT, preferred_element_type=F32
        )

    def main_dots(l, pos, c, accs):
        return tuple(
            acc + jnp.dot(scaled[pos], ref[l, at_chip(c), :], preferred_element_type=F32)
            for acc, ref in zip(accs, (wg, wv, ws))
        )

    def send_keys(l, key_acc, squares):
        inv_scale = lax.rsqrt(jnp.sum(squares, axis=1, keepdims=True) / depth + EPS)
        key_in = key_acc * inv_scale
        mixed = []
        for i in range(2):
            fresh = key_in[:, i * key_cols : (i + 1) * key_cols]
            total = fresh * ckw[l, TAPS - 1, i : i + 1, :]
            for k in range(TAPS - 1):
                total = total + ck[l, :, k, i, :] * ckw[l, k, i : i + 1, :]
            mixed.append(silu(total))
        mixed = jnp.concatenate(
            mixed + [jnp.zeros((batch, LANES - 2 * key_cols), F32)], axis=1
        )
        spread = jnp.concatenate([mixed] * own_entries, axis=0).T
        lane_entry = iota((GROUPS, LANES), 1) // batch
        for i in range(2):
            packed = jnp.zeros((GROUPS, LANES), F32)
            for e in range(own_entries):
                at = (i * own_entries + e) * GROUPS
                packed = jnp.where(lane_entry == e, spread[at : at + GROUPS], packed)
            keys_send[l, :, i, :] = packed
        keys_recv[l, me] = keys_send[l, my_group]
        if l == 0:
            pl.semaphore_wait(barrier, n - 1)
        for m in far:
            for to in ([2 * chip_of[m], 2 * chip_of[m] + 1] if m else [buddy]):
                remote(
                    keys_send.at[l, to // peers], keys_recv.at[l, me], key_ss, key_rs, to
                ).start()
        return inv_scale, key_in

    zeros = tuple(jnp.zeros((batch, ref.shape[2]), F32) for ref in (wg, wv, ws))
    key_zero = jnp.zeros((batch, 2 * key_cols), F32)
    square_zero = jnp.zeros((batch, block), F32)

    quarter = chips // 4
    waves = [near[q * quarter : (q + 1) * quarter] for q in range(4)]
    wave_of = {m: q for q, wave in enumerate(waves) for m in wave}

    def blocks(l, count):
        return hidden.at[l, pl.ds(0, count)]

    def forward_wave(l, q):
        remote(blocks(l, quarter), blocks(l, quarter), ag_ss, ag_rs.at[q], buddy).wait_recv()
        for m in waves[q]:
            if m:
                at = hidden.at[l, 2 * chip_of[m] + other]
                remote(at, at, fw_ss, fw_rs.at[q], buddy).start()

    def whole(l, q):
        count = sum(1 for m in waves[q] if m)
        remote(blocks(l, count), blocks(l, count), fw_ss, fw_rs.at[q], buddy).wait_recv()

    def sent(src, sem):
        remote(src, src, sem, rs_rs, buddy).wait_send()

    for l in range(layers):
        if l == 0:
            for copy in big[0][2:5] + small[4:]:
                copy.start()
            for copy in small[:4] + big[0][:2]:
                copy.wait()
            squares = square_zero
            key_acc = key_zero
            for c in range(chips):
                squares = prepare(l, c, c, squares)
                key_acc = key_dot(l, c, c, key_acc)
            inv_scale, key_in = send_keys(l, key_acc, squares)
            for copy in big[0][5:]:
                copy.start()
            for copy in big[0][2:5]:
                copy.wait()
            accs = zeros
            for c in range(chips):
                accs = main_dots(l, c, c, accs)
            for copy in small[4:]:
                copy.wait()
        else:
            for copy in big[l][:5]:
                copy.wait()
            squares, key_acc, accs = square_zero, key_zero, zeros
            for q in range(4):
                forward_wave(l - 1, q)
            for q, wave in enumerate(waves):
                whole(l - 1, q)
                for i, m in enumerate(wave):
                    pos = q * quarter + i
                    squares = prepare(l, pos, chip_of[m], squares)
                    key_acc = key_dot(l, pos, chip_of[m], key_acc)
            inv_scale, key_in = send_keys(l, key_acc, squares)
            for pos, m in enumerate(near):
                accs = main_dots(l, pos, chip_of[m], accs)
        gate_in, value_in, step_in = [acc * inv_scale for acc in accs]
        for i in range(2):
            for k in range(1, TAPS - 1):
                key_out[l, :, k - 1, i, :] = ck[l, :, k, i, :]
            key_out[l, :, TAPS - 2, i, :] = key_in[:, i * key_cols : (i + 1) * key_cols]
        for k in range(1, TAPS - 1):
            value_out[l, :, k - 1, :] = cv[l, :, k, :]
        value_out[l, :, TAPS - 2, :] = value_in
        values = value_in * cvw[TAPS - 1, l : l + 1, :]
        for k in range(TAPS - 1):
            values = values + cv[l, :, k, :] * cvw[k, l : l + 1, :]
        values = silu(values)
        raw = step_in + bias[l : l + 1, :]
        delta = jnp.maximum(raw, 0.0) + jnp.log1p(jnp.exp(-jnp.abs(raw)))
        decay = jnp.exp(-delta * rate[l : l + 1, :])
        skips = jnp.broadcast_to(skip[l : l + 1, :], (8, heads))
        chan = select_dot(jnp.concatenate([delta, decay, skips], axis=0), head_hot)
        decay_chan = chan[batch : 2 * batch]
        skip_chan = chan[2 * batch : 2 * batch + 1]
        dv = chan[:batch] * values
        cols[...] = jnp.concatenate(
            [dv, decay_chan, jnp.zeros((LANES - 2 * batch, chans), F32)], axis=0
        ).T
        gate = silu(gate_in)
        big[l][5].wait()
        if l:
            sent(rs_send.at[l - 1], rs_ss)
            sent(blocks(l - 1, chips), ag_ss)
            sent(blocks(l - 1, chips - 1), fw_ss)

        def turn(g, carry):
            for j in range(4):
                turned[4 * g + j] = state[l, 4 * g + j].T.astype(BF16)
            return carry

        lax.fori_loop(0, batch // 4, turn, 0)
        big[l][6].wait()

        remote(
            keys_recv.at[l, pl.ds(0, n - 1)], keys_recv.at[l, pl.ds(0, n - 1)],
            key_ss, key_rs, buddy,
        ).wait_recv()
        arrived = keys_recv[l].reshape(2 * n, LANES)
        arrived = jnp.concatenate([arrived, arrived], axis=0).T
        left_half = iota((batch, LANES), 1) < LANES // 2
        pieces = [
            jnp.where(
                left_half,
                arrived[2 * h * batch : (2 * h + 1) * batch],
                arrived[(2 * h + 1) * batch : (2 * h + 2) * batch],
            )
            for h in range(2)
        ]
        both = select_dot(jnp.concatenate(pieces, axis=1), recv_hot)
        writes = both[:, :entries]
        reads = both[:, entries:]
        wbuf[...] = writes
        lane_half = iota((8, 2 * entries), 1) // entries
        sub = iota((8, 2 * entries), 0)
        query = []
        for g in range(groups8):
            reads8 = reads[8 * g : 8 * g + 8]
            twice = jnp.concatenate([reads8, reads8], axis=1)
            total = jnp.zeros((8, chans), F32)
            for p in range(4):
                left = jnp.where(sub == 2 * p + lane_half, twice, 0.0).astype(BF16)
                right = turned[pl.ds(8 * g + 2 * p, 2)].reshape(2 * entries, chans)
                total = total + jnp.dot(left, right, preferred_element_type=F32)
            query.append(total)
        query = jnp.concatenate(query, axis=0)
        through = jnp.sum(writes * reads, axis=1, keepdims=True)
        mixed_out = decay_chan * query + dv * through + skip_chan * values
        gated = mixed_out * gate
        fed = (gated * gg[l : l + 1, :]).astype(BF16)

        def out_pair(i, parity):
            rhs = jnp.concatenate(
                [
                    wo[l, :, pl.ds(pl.multiple_of((2 * chip_of[far[i + j]] + parity) * LANES, LANES), LANES)]
                    for j in range(2)
                ],
                axis=1,
            )
            return jnp.dot(fed, rhs, preferred_element_type=F32)

        square = gated * gated
        square = square[:, :LANES] + square[:, LANES:]
        square = jnp.concatenate([square, jnp.zeros((LANES - batch, LANES), F32)], axis=0).T
        sq_own[l] = jnp.sum(square, axis=0, keepdims=True)
        sp_copy = remote(sq_own.at[l], sq_pair.at[l], sp_ss, sp_rs, buddy)
        sp_copy.start()

        def pair_copy(q):
            at = pl.ds(q * quarter, quarter)
            return remote(pair_send.at[l, at], pair_recv.at[l, at], pair_ss, pair_rs.at[q], buddy)

        for q in range(4):
            for i in range(q * quarter, (q + 1) * quarter, 2):
                res = out_pair(i, core).astype(BF16)
                pair_send[l, i] = res[:, :LANES]
                pair_send[l, i + 1] = res[:, LANES:]
            pair_copy(q).start()
        for i in range(0, chips, 2):
            res = out_pair(i, other)
            part[i] = res[:, :LANES]
            part[i + 1] = res[:, LANES:]
        sp_copy.wait_recv()
        sq_send[l] = sq_own[l] + sq_pair[l]
        for m in far:
            remote(
                sq_send.at[l], sq_recv.at[l, chip], sq_ss, sq_rs, 2 * chip_of[m] + other
            ).start()

        def rs_copy(i):
            return remote(
                rs_send.at[l, i], rs_recv.at[l, chip], rs_ss, rs_rs, 2 * chip_of[far[i]] + other
            )

        for q in range(4):
            pair_copy(q).wait_recv()
            for i in range(q * quarter, (q + 1) * quarter):
                rs_send[l, i] = (part[i] + pair_recv[l, i].astype(F32)).astype(BF16)
                rs_copy(i).start()
        if l + 1 < layers:
            for copy in big[l + 1]:
                copy.start()
        update_range(l, 0, groups8)
        sent(keys_recv.at[l, pl.ds(0, n - 1)], key_ss)
        sent(sq_own.at[l], sp_ss)
        sent(pair_send.at[l], pair_ss)
        sent(sq_recv.at[l], sq_ss)
        remote(sq_recv.at[l], sq_recv.at[l], sq_ss, sq_rs, buddy).wait_recv()
        rows = []
        for g in range(GROUPS):
            total = sq_recv[l, per_group * g]
            for k in range(1, per_group):
                total = total + sq_recv[l, per_group * g + k]
            rows.append(total)
        rows = lax.rsqrt(jnp.concatenate(rows, axis=0) / GW + EPS)
        columns = jnp.concatenate([rows, jnp.zeros((LANES - GROUPS, LANES), F32)], axis=0).T
        for g in range(GROUPS):
            scales[g] = jnp.broadcast_to(columns[:batch, g : g + 1], (batch, LANES))
        if l == 0:
            resid = tokens[:, pl.ds(pl.multiple_of(me * LANES, LANES), LANES)]
        else:
            resid = hidden[l - 1, me]
        remote(rs_recv.at[l], rs_recv.at[l], rs_ss, rs_rs, buddy).wait_recv()
        sums = [resid.astype(F32)] + [jnp.zeros((batch, LANES), F32)] * 3
        for g in range(GROUPS):
            term = rs_recv[l, per_group * g].astype(F32)
            for k in range(1, per_group):
                term = term + rs_recv[l, per_group * g + k].astype(F32)
            sums[g % 4] = sums[g % 4] + term * scales[g]
        hidden[l, me] = ((sums[0] + sums[1]) + (sums[2] + sums[3])).astype(BF16)
        for m in far:
            remote(
                hidden.at[l, me], hidden.at[l, me], ag_ss, ag_rs.at[wave_of[m]], 2 * chip_of[m] + other
            ).start()

    for q in range(4):
        forward_wave(layers - 1, q)
    for q in range(4):
        whole(layers - 1, q)
    for j in range(n):
        tokens_out[:, j * LANES : (j + 1) * LANES] = hidden[layers - 1, j]
    sent(rs_send.at[layers - 1], rs_ss)
    sent(blocks(layers - 1, chips), ag_ss)
    sent(blocks(layers - 1, chips - 1), fw_ss)


def flush(tokens, state, value, key, tokens_hbm, state_hbm, value_hbm, key_hbm, sems):
    layers, batch = state.shape[:2]
    step = batch // 4
    copies = [
        pltpu.make_async_copy(key, key_hbm, sems.at[0]),
        pltpu.make_async_copy(value, value_hbm, sems.at[1]),
        pltpu.make_async_copy(tokens, tokens_hbm, sems.at[2]),
    ]
    for l in range(layers):
        for i in range(4):
            at = pl.ds(i * step, step)
            copies.append(
                pltpu.make_async_copy(state.at[l, at], state_hbm.at[l, at], sems.at[len(copies)])
            )
    for copy in copies:
        copy.start()
    for copy in copies:
        copy.wait()


def fused(n, *args):
    (tokens, norm_gain, w_gate, w_value, w_write, w_read, w_step, step_bias, decay_rate) = args[:9]
    (skip_gain, cvw, ckw, group_gain, w_out, ssm_state, conv_value, conv_key) = args[9:]
    layers, batch, chans, entries = ssm_state.shape
    depth = tokens.shape[1]
    chips = n // 2
    key_cols = w_write.shape[2]
    operands = list(args)
    operands[4] = jnp.swapaxes(w_write, 1, 2)
    operands[5] = jnp.swapaxes(w_read, 1, 2)
    operands[10] = jnp.swapaxes(cvw, 0, 1)
    landed = [pltpu.VMEM(a.shape, a.dtype) for a in operands]
    landed[4:6] = [pltpu.VMEM((layers, 2 * key_cols, depth), BF16)]
    del landed[13]
    dma = pltpu.SemaphoreType.DMA
    outs = (
        jax.ShapeDtypeStruct(tokens.shape, BF16),
        jax.ShapeDtypeStruct(ssm_state.shape, F32),
        jax.ShapeDtypeStruct(conv_value.shape, F32),
        jax.ShapeDtypeStruct(conv_key.shape, F32),
    )
    small_bytes = 4 * 1024 * 1024
    results = pl.pallas_call(
        functools.partial(mixer, n),
        out_shape=tuple(pltpu.VMEM(o.shape, o.dtype) for o in outs),
        in_specs=[pl.BlockSpec(memory_space=pltpu.HBM)] * len(operands),
        out_specs=(pl.BlockSpec(memory_space=pltpu.VMEM),) * 4,
        scratch_shapes=landed
        + [
            pltpu.VMEM((layers, n, batch, LANES), BF16),
            pltpu.VMEM((chips, batch, depth // chips), BF16),
            pltpu.VMEM((layers, GROUPS, 2, LANES), F32),
            pltpu.VMEM((layers, n, 2, LANES), F32),
            pltpu.VMEM((layers, chips, batch, LANES), BF16),
            pltpu.VMEM((layers, chips, batch, LANES), BF16),
            pltpu.VMEM((chips, batch, LANES), F32),
            pltpu.VMEM((layers, chips, batch, LANES), BF16),
            pltpu.VMEM((layers, chips, batch, LANES), BF16),
            pltpu.VMEM((layers, 1, LANES), F32),
            pltpu.VMEM((layers, 1, LANES), F32),
            pltpu.VMEM((layers, 1, LANES), F32),
            pltpu.VMEM((layers, chips, 1, LANES), F32),
            pltpu.VMEM((GROUPS, batch, LANES), F32),
            pltpu.VMEM((batch, entries, chans), BF16),
            pltpu.VMEM((chans, LANES), F32),
            pltpu.VMEM((batch, entries), F32),
            dma((17,)),
            dma((7,)),
            dma((4,)),
            dma((4,)),
            dma((4,)),
            dma((4,)),
        ],
        compiler_params=pltpu.CompilerParams(
            collective_id=0,
            has_side_effects=True,
            vmem_limit_bytes=VMEM - ssm_state.size * 4 - small_bytes,
        ),
        name="mixer",
    )(*operands)
    return pl.pallas_call(
        flush,
        out_shape=outs,
        in_specs=[pl.BlockSpec(memory_space=pl.ANY)] * 4,
        out_specs=(pl.BlockSpec(memory_space=pltpu.HBM),) * 4,
        scratch_shapes=[dma((3 + 4 * layers,))],
        compiler_params=pltpu.CompilerParams(vmem_limit_bytes=1024 * 1024),
        name="flush",
    )(*results)


def dispatch(n, *args):
    depth = args[0].shape[1]
    layers, batch, chans, entries = args[14].shape
    own_entries = args[4].shape[2] // GROUPS
    fits = (
        depth == n * LANES
        and n == 32
        and own_entries == 4
        and own_entries * batch == LANES
        and entries == LANES
        and chans == 2 * LANES
        and args[7].shape[1] == LANES
    )
    return fused(n, *args) if fits else per_device(*args)


def solution(mesh):
    placed = (
        P(),
        P(),
        P(None, None, "tp"),
        P(None, None, "tp"),
        P(None, None, "tp"),
        P(None, None, "tp"),
        P(),
        P(),
        P(),
        P(),
        P(None, None, "tp"),
        P(None, None, None, "tp"),
        P(None, "tp"),
        P(None, "tp", None),
        P(None, None, "tp", None),
        P(None, None, None, "tp"),
        P(None, None, None, None, "tp"),
    )
    return jax.shard_map(
        functools.partial(dispatch, mesh.shape["tp"]),
        mesh=mesh,
        in_specs=placed,
        out_specs=(
            P(),
            P(None, None, "tp", None),
            P(None, None, None, "tp"),
            P(None, None, None, None, "tp"),
        ),
        check_vma=False,
    )
```

```python
import jax
import jax.numpy as jnp
from jax import lax
from jax.experimental import pallas as pl
from jax.experimental.pallas import tpu as pltpu
from jax.sharding import PartitionSpec as P
import functools

D = 4096
HEAD_DIM = 64
GROUPS = 8
STATE = 128
LAYERS = 2
HEADS = 128
GW = 1024


EPS = 1e-06


def per_device(
    tokens,
    norm_gain,
    w_gate,
    w_value,
    w_write,
    w_read,
    w_step,
    step_bias,
    decay_rate,
    skip_gain,
    conv_value_weight,
    conv_key_weight,
    group_gain,
    w_out,
    ssm_state,
    conv_value,
    conv_key,
):
    highest = lax.Precision.HIGHEST
    chan_count = w_gate.shape[2]
    position = lax.axis_index("tp")
    first_chan = position * chan_count
    chan_ids = first_chan + jnp.arange(chan_count, dtype=jnp.int32)
    my_group = first_chan // GW
    head_hot = (
        (chan_ids // HEAD_DIM)[:, None] == jnp.arange(HEADS, dtype=jnp.int32)[None, :]
    ).astype(jnp.float32)
    group_hot = ((chan_ids // GW)[:, None] == jnp.arange(GROUPS, dtype=jnp.int32)[None, :]).astype(
        jnp.float32
    )
    hidden = tokens
    ssm_list = []
    value_list = []
    key_list = []
    for layer in range(LAYERS):
        resid = hidden.astype(jnp.float32)
        inv_scale = lax.rsqrt(jnp.sum(resid * resid, axis=1) / D + EPS)[:, None]
        scaled = (resid * norm_gain[layer]).astype(jnp.bfloat16)

        def project(weight):
            return jnp.dot(scaled, weight[layer], preferred_element_type=jnp.float32) * inv_scale

        gate_in = project(w_gate)
        value_in = project(w_value)
        write_in = project(w_write)
        read_in = project(w_read)
        step_in = project(w_step)
        value_window = jnp.concatenate([conv_value[layer], value_in[:, None, :]], axis=1)
        value_list.append(value_window[:, 1:])
        values = jax.nn.silu(jnp.sum(value_window * conv_value_weight[layer][None], axis=1))
        fresh = jnp.stack([write_in, read_in], axis=1)[:, None]
        key_window = jnp.concatenate([conv_key[layer], fresh], axis=1)
        key_list.append(key_window[:, 1:])
        mixed_keys = jax.nn.silu(jnp.sum(key_window * conv_key_weight[layer][None], axis=1))
        every_group = lax.all_gather(mixed_keys, "tp", axis=2, tiled=True)
        by_entry = every_group.reshape(every_group.shape[0], 2, STATE, GROUPS)
        own_keys = lax.dynamic_slice_in_dim(by_entry, my_group, 1, 3)[..., 0]
        writes = own_keys[:, 0]
        reads = own_keys[:, 1]
        delta = jax.nn.softplus(step_in + step_bias[layer][None])
        decay = jnp.exp(-delta * decay_rate[layer][None])
        delta_chan = jnp.dot(delta, head_hot.T, precision=highest)
        decay_chan = jnp.dot(decay, head_hot.T, precision=highest)
        skip_chan = jnp.dot(skip_gain[layer], head_hot.T, precision=highest)
        state = (
            decay_chan[..., None] * ssm_state[layer]
            + (delta_chan * values)[..., None] * writes[:, None, :]
        )
        ssm_list.append(state)
        read_out = jnp.sum(state * reads[:, None, :], axis=2) + skip_chan[None] * values
        gated = read_out * jax.nn.silu(gate_in)
        squares = jnp.dot(gated * gated, group_hot, precision=highest)
        square_total = lax.psum(squares, "tp")
        group_scale = lax.rsqrt(square_total / GW + EPS)
        scale_chan = jnp.dot(group_scale, group_hot.T, precision=highest)
        normed = (gated * scale_chan * group_gain[layer][None]).astype(jnp.bfloat16)
        partial_out = jnp.dot(normed, w_out[layer], preferred_element_type=jnp.float32)
        update = lax.psum(partial_out, "tp")
        hidden = (resid + update).astype(jnp.bfloat16)
    return (hidden, jnp.stack(ssm_list), jnp.stack(value_list), jnp.stack(key_list))


LANES = 128
TAPS = 3
VMEM = 67043328
BF16 = jnp.bfloat16
F32 = jnp.float32
NT = (((1,), (1,)), ((), ()))


def split3(x):
    high = x.astype(BF16)
    rest = x - high.astype(F32)
    mid = rest.astype(BF16)
    return high, mid, (rest - mid.astype(F32)).astype(BF16)


def select_dot(x, hot):
    rows = x.shape[0]
    parts = jnp.concatenate(split3(x), axis=0)
    out = jnp.dot(parts, hot, preferred_element_type=F32)
    return out[:rows] + out[rows : 2 * rows] + out[2 * rows :]


def silu(v):
    return v / (1.0 + jnp.exp(-v))


def iota(shape, axis):
    return lax.broadcasted_iota(jnp.int32, shape, axis)


def mixer(
    n,
    tokens_hbm,
    gain_hbm,
    wg_hbm,
    wv_hbm,
    ww_hbm,
    wr_hbm,
    ws_hbm,
    bias_hbm,
    rate_hbm,
    skip_hbm,
    cvw_hbm,
    ckw_hbm,
    gg_hbm,
    wo_hbm,
    state_hbm,
    cv_hbm,
    ck_hbm,
    tokens_out,
    state,
    value_out,
    key_out,
    tokens,
    gain,
    wg,
    wv,
    wk,
    ws,
    bias,
    rate,
    skip,
    cvw,
    ckw,
    gg,
    wo,
    cv,
    ck,
    hidden,
    scaled,
    keys_send,
    keys_recv,
    pair_send,
    pair_recv,
    part,
    rs_send,
    rs_recv,
    sq_own,
    sq_pair,
    sq_send,
    sq_recv,
    scales,
    turned,
    cols,
    wbuf,
    in_sem,
    send_sem,
    recv_sem,
    pair_rs,
    ag_rs,
    fw_rs,
):
    key_ss, pair_ss, rs_ss, ag_ss, fw_ss, sp_ss, sq_ss = [send_sem.at[i] for i in range(7)]
    key_rs, sp_rs, sq_rs, rs_rs = [recv_sem.at[i] for i in range(4)]
    layers, batch, chans, entries = state.shape
    depth = tokens.shape[1]
    chips = n // 2
    block = depth // chips
    key_cols = wk.shape[1] // 2
    own_entries = key_cols // GROUPS
    heads = bias.shape[1]
    peers = GW // chans
    per_group = peers // 2
    me = lax.axis_index("tp")
    chip = me // 2
    core = lax.rem(me, 2)
    other = 1 - core
    buddy = 2 * chip + other
    my_group = me // peers

    small_pairs = (
        (tokens_hbm, tokens),
        (gain_hbm, gain),
        (ck_hbm, ck),
        (ckw_hbm, ckw),
        (bias_hbm, bias),
        (rate_hbm, rate),
        (skip_hbm, skip),
        (cvw_hbm, cvw),
        (gg_hbm, gg),
        (cv_hbm, cv),
    )
    small = [pltpu.make_async_copy(a, b, in_sem.at[i]) for i, (a, b) in enumerate(small_pairs)]
    big = [
        [
            pltpu.make_async_copy(a.at[l], b.at[l], in_sem.at[len(small_pairs) + i])
            for i, (a, b) in enumerate(
                (
                    (ww_hbm, wk.at[:, :key_cols]),
                    (wr_hbm, wk.at[:, key_cols:]),
                    (wg_hbm, wg),
                    (wv_hbm, wv),
                    (ws_hbm, ws),
                    (state_hbm, state),
                    (wo_hbm, wo),
                )
            )
        ]
        for l in range(layers)
    ]
    for copy in small[:4] + big[0][:2]:
        copy.start()

    def flipped(value, mask):
        bit = 1
        out = value
        while bit <= mask:
            if mask & bit:
                out = out + bit - 2 * bit * lax.rem(value // bit, 2)
            bit *= 2
        return out

    chip_of = [flipped(chip, m) for m in range(chips)]

    def distance(m):
        return (m >> 2) + (m >> 1) % 2 + m % 2

    far = sorted(range(chips), key=lambda m: (-distance(m), m))
    near = far[::-1]

    barrier = pltpu.get_barrier_semaphore()

    def signal(to):
        pl.semaphore_signal(barrier, inc=1, device_id=(to,), device_id_type=pl.DeviceIdType.MESH)

    for m in far[:-1]:
        signal(2 * chip_of[m])
        signal(2 * chip_of[m] + 1)
    signal(buddy)

    def remote(src, dst, ss, rs, to):
        return pltpu.make_async_remote_copy(
            src_ref=src,
            dst_ref=dst,
            send_sem=ss,
            recv_sem=rs,
            device_id=(to,),
            device_id_type=pl.DeviceIdType.MESH,
        )

    senders = entries // own_entries
    row = iota((entries, entries), 0)
    col = iota((entries, entries), 1)
    natural = jnp.where(
        col == (row % senders) * own_entries + row // senders, 1.0, 0.0
    ).astype(BF16)
    row = iota((heads, chans), 0)
    col = iota((heads, chans), 1)
    head_hot = jnp.where(row == (me * chans + col) // HEAD_DIM, 1.0, 0.0).astype(BF16)

    groups8 = batch // 8

    def update_state(l, group):
        shifted = pltpu.roll(cols[...], lax.rem(LANES - 8 * group, LANES), 1)
        writes8 = wbuf[pl.ds(pl.multiple_of(8 * group, 8), 8), :]
        for j in range(8):
            b = 8 * group + j
            state[l, b] = (
                shifted[:, batch + j : batch + j + 1] * state[l, b]
                + shifted[:, j : j + 1] * writes8[j : j + 1, :]
            )

    def update_range(l, low, high):
        def step(g, carry):
            update_state(l, g)
            return carry

        lax.fori_loop(low, high, step, 0)

    def at_chip(c):
        return pl.ds(pl.multiple_of(c * block, block), block)

    def prepare(l, pos, c, squares):
        if l == 0:
            x = tokens[:, at_chip(c)].astype(F32)
        else:
            x = jnp.concatenate([hidden[l - 1, 2 * c], hidden[l - 1, 2 * c + 1]], axis=1).astype(F32)
        scaled[pos] = (x * gain[l : l + 1, at_chip(c)]).astype(BF16)
        return squares + x * x

    def key_dot(l, pos, c, acc):
        return acc + lax.dot_general(
            scaled[pos], wk[l, :, at_chip(c)], NT, preferred_element_type=F32
        )

    def main_dots(l, pos, c, accs):
        return tuple(
            acc + jnp.dot(scaled[pos], ref[l, at_chip(c), :], preferred_element_type=F32)
            for acc, ref in zip(accs, (wg, wv, ws))
        )

    def send_keys(l, key_acc, squares):
        inv_scale = lax.rsqrt(jnp.sum(squares, axis=1, keepdims=True) / depth + EPS)
        key_in = key_acc * inv_scale
        mixed = []
        for i in range(2):
            fresh = key_in[:, i * key_cols : (i + 1) * key_cols]
            total = fresh * ckw[l, TAPS - 1, i : i + 1, :]
            for k in range(TAPS - 1):
                total = total + ck[l, :, k, i, :] * ckw[l, k, i : i + 1, :]
            mixed.append(silu(total))
        mixed = jnp.concatenate(
            mixed + [jnp.zeros((batch, LANES - 2 * key_cols), F32)], axis=1
        )
        spread = jnp.concatenate([mixed] * own_entries, axis=0).T
        lane_entry = iota((GROUPS, LANES), 1) // batch
        for i in range(2):
            packed = jnp.zeros((GROUPS, LANES), F32)
            for e in range(own_entries):
                at = (i * own_entries + e) * GROUPS
                packed = jnp.where(lane_entry == e, spread[at : at + GROUPS], packed)
            keys_send[l, :, i, :] = packed
        keys_recv[l, me] = keys_send[l, my_group]
        if l == 0:
            pl.semaphore_wait(barrier, n - 1)
        for m in far:
            for to in ([2 * chip_of[m], 2 * chip_of[m] + 1] if m else [buddy]):
                remote(
                    keys_send.at[l, to // peers], keys_recv.at[l, me], key_ss, key_rs, to
                ).start()
        return inv_scale, key_in

    zeros = tuple(jnp.zeros((batch, ref.shape[2]), F32) for ref in (wg, wv, ws))
    key_zero = jnp.zeros((batch, 2 * key_cols), F32)
    square_zero = jnp.zeros((batch, block), F32)

    quarter = chips // 4
    waves = [near[q * quarter : (q + 1) * quarter] for q in range(4)]
    wave_of = {m: q for q, wave in enumerate(waves) for m in wave}

    def blocks(l, count):
        return hidden.at[l, pl.ds(0, count)]

    def forward_wave(l, q):
        remote(blocks(l, quarter), blocks(l, quarter), ag_ss, ag_rs.at[q], buddy).wait_recv()
        for m in waves[q]:
            if m:
                at = hidden.at[l, 2 * chip_of[m] + other]
                remote(at, at, fw_ss, fw_rs.at[q], buddy).start()

    def whole(l, q):
        count = sum(1 for m in waves[q] if m)
        remote(blocks(l, count), blocks(l, count), fw_ss, fw_rs.at[q], buddy).wait_recv()

    def sent(src, sem):
        remote(src, src, sem, rs_rs, buddy).wait_send()

    for l in range(layers):
        if l == 0:
            for copy in big[0][2:5] + small[4:]:
                copy.start()
            for copy in small[:4] + big[0][:2]:
                copy.wait()
            squares = square_zero
            key_acc = key_zero
            for c in range(chips):
                squares = prepare(l, c, c, squares)
                key_acc = key_dot(l, c, c, key_acc)
            inv_scale, key_in = send_keys(l, key_acc, squares)
            for copy in big[0][5:]:
                copy.start()
            for copy in big[0][2:5]:
                copy.wait()
            accs = zeros
            for c in range(chips):
                accs = main_dots(l, c, c, accs)
            for copy in small[4:]:
                copy.wait()
        else:
            for copy in big[l][:5]:
                copy.wait()
            squares, key_acc, accs = square_zero, key_zero, zeros
            for q in range(4):
                forward_wave(l - 1, q)
            for q, wave in enumerate(waves):
                whole(l - 1, q)
                for i, m in enumerate(wave):
                    pos = q * quarter + i
                    squares = prepare(l, pos, chip_of[m], squares)
                    key_acc = key_dot(l, pos, chip_of[m], key_acc)
            inv_scale, key_in = send_keys(l, key_acc, squares)
            for pos, m in enumerate(near):
                accs = main_dots(l, pos, chip_of[m], accs)
        gate_in, value_in, step_in = [acc * inv_scale for acc in accs]
        for i in range(2):
            for k in range(1, TAPS - 1):
                key_out[l, :, k - 1, i, :] = ck[l, :, k, i, :]
            key_out[l, :, TAPS - 2, i, :] = key_in[:, i * key_cols : (i + 1) * key_cols]
        for k in range(1, TAPS - 1):
            value_out[l, :, k - 1, :] = cv[l, :, k, :]
        value_out[l, :, TAPS - 2, :] = value_in
        values = value_in * cvw[TAPS - 1, l : l + 1, :]
        for k in range(TAPS - 1):
            values = values + cv[l, :, k, :] * cvw[k, l : l + 1, :]
        values = silu(values)
        raw = step_in + bias[l : l + 1, :]
        delta = jnp.maximum(raw, 0.0) + jnp.log1p(jnp.exp(-jnp.abs(raw)))
        decay = jnp.exp(-delta * rate[l : l + 1, :])
        skips = jnp.broadcast_to(skip[l : l + 1, :], (8, heads))
        chan = select_dot(jnp.concatenate([delta, decay, skips], axis=0), head_hot)
        decay_chan = chan[batch : 2 * batch]
        skip_chan = chan[2 * batch : 2 * batch + 1]
        dv = chan[:batch] * values
        cols[...] = jnp.concatenate(
            [dv, decay_chan, jnp.zeros((LANES - 2 * batch, chans), F32)], axis=0
        ).T
        gate = silu(gate_in)
        big[l][5].wait()
        if l:
            sent(rs_send.at[l - 1], rs_ss)
            sent(blocks(l - 1, chips), ag_ss)
            sent(blocks(l - 1, chips - 1), fw_ss)

        def turn(g, carry):
            for j in range(8):
                turned[8 * g + j] = lax.dot_general(
                    natural, state[l, 8 * g + j].astype(BF16), NT, preferred_element_type=F32
                ).astype(BF16)
            return carry

        lax.fori_loop(0, groups8, turn, 0)
        big[l][6].wait()

        remote(
            keys_recv.at[l, pl.ds(0, n - 1)], keys_recv.at[l, pl.ds(0, n - 1)],
            key_ss, key_rs, buddy,
        ).wait_recv()
        lane_entry = iota((batch, LANES), 1) // senders
        grouped = []
        for i in range(2):
            arrived = jnp.concatenate([keys_recv[l, :, i, :]] * own_entries, axis=0).T
            rows = arrived[:batch]
            for e in range(1, own_entries):
                rows = jnp.where(lane_entry == e, arrived[e * batch : (e + 1) * batch], rows)
            grouped.append(rows)
        writes, reads = grouped
        lane_half = iota((8, 2 * entries), 1) // entries
        sub = iota((8, 2 * entries), 0)
        query = []
        for g in range(groups8):
            reads8 = reads[8 * g : 8 * g + 8]
            twice = jnp.concatenate([reads8, reads8], axis=1)
            total = jnp.zeros((8, chans), F32)
            for p in range(4):
                left = jnp.where(sub == 2 * p + lane_half, twice, 0.0).astype(BF16)
                right = turned[pl.ds(8 * g + 2 * p, 2)].reshape(2 * entries, chans)
                total = total + jnp.dot(left, right, preferred_element_type=F32)
            query.append(total)
        query = jnp.concatenate(query, axis=0)
        through = jnp.sum(writes * reads, axis=1, keepdims=True)
        mixed_out = decay_chan * query + dv * through + skip_chan * values
        gated = mixed_out * gate
        fed = (gated * gg[l : l + 1, :]).astype(BF16)

        def out_pair(i, parity):
            rhs = jnp.concatenate(
                [
                    wo[l, :, pl.ds(pl.multiple_of((2 * chip_of[far[i + j]] + parity) * LANES, LANES), LANES)]
                    for j in range(2)
                ],
                axis=1,
            )
            return jnp.dot(fed, rhs, preferred_element_type=F32)

        square = gated * gated
        square = square[:, :LANES] + square[:, LANES:]
        square = jnp.concatenate([square, jnp.zeros((LANES - batch, LANES), F32)], axis=0).T
        sq_own[l] = jnp.sum(square, axis=0, keepdims=True)
        sp_copy = remote(sq_own.at[l], sq_pair.at[l], sp_ss, sp_rs, buddy)
        sp_copy.start()

        def pair_copy(q):
            at = pl.ds(q * quarter, quarter)
            return remote(pair_send.at[l, at], pair_recv.at[l, at], pair_ss, pair_rs.at[q], buddy)

        for q in range(4):
            for i in range(q * quarter, (q + 1) * quarter, 2):
                res = out_pair(i, core).astype(BF16)
                pair_send[l, i] = res[:, :LANES]
                pair_send[l, i + 1] = res[:, LANES:]
            pair_copy(q).start()
        for i in range(0, chips, 2):
            res = out_pair(i, other)
            part[i] = res[:, :LANES]
            part[i + 1] = res[:, LANES:]
        sp_copy.wait_recv()
        sq_send[l] = sq_own[l] + sq_pair[l]
        for m in far:
            remote(
                sq_send.at[l], sq_recv.at[l, chip], sq_ss, sq_rs, 2 * chip_of[m] + other
            ).start()

        def rs_copy(i):
            return remote(
                rs_send.at[l, i], rs_recv.at[l, chip], rs_ss, rs_rs, 2 * chip_of[far[i]] + other
            )

        for q in range(4):
            pair_copy(q).wait_recv()
            for i in range(q * quarter, (q + 1) * quarter):
                rs_send[l, i] = (part[i] + pair_recv[l, i].astype(F32)).astype(BF16)
                rs_copy(i).start()
        if l + 1 < layers:
            for copy in big[l + 1]:
                copy.start()
        wbuf[...] = select_dot(writes, natural)
        update_range(l, 0, groups8)
        sent(keys_recv.at[l, pl.ds(0, n - 1)], key_ss)
        sent(sq_own.at[l], sp_ss)
        sent(pair_send.at[l], pair_ss)
        sent(sq_recv.at[l], sq_ss)
        remote(sq_recv.at[l], sq_recv.at[l], sq_ss, sq_rs, buddy).wait_recv()
        rows = []
        for g in range(GROUPS):
            total = sq_recv[l, per_group * g]
            for k in range(1, per_group):
                total = total + sq_recv[l, per_group * g + k]
            rows.append(total)
        rows = lax.rsqrt(jnp.concatenate(rows, axis=0) / GW + EPS)
        columns = jnp.concatenate([rows, jnp.zeros((LANES - GROUPS, LANES), F32)], axis=0).T
        for g in range(GROUPS):
            scales[g] = jnp.broadcast_to(columns[:batch, g : g + 1], (batch, LANES))
        if l == 0:
            resid = tokens[:, pl.ds(pl.multiple_of(me * LANES, LANES), LANES)]
        else:
            resid = hidden[l - 1, me]
        remote(rs_recv.at[l], rs_recv.at[l], rs_ss, rs_rs, buddy).wait_recv()
        sums = [resid.astype(F32)] + [jnp.zeros((batch, LANES), F32)] * 3
        for g in range(GROUPS):
            term = rs_recv[l, per_group * g].astype(F32)
            for k in range(1, per_group):
                term = term + rs_recv[l, per_group * g + k].astype(F32)
            sums[g % 4] = sums[g % 4] + term * scales[g]
        hidden[l, me] = ((sums[0] + sums[1]) + (sums[2] + sums[3])).astype(BF16)
        for m in far:
            remote(
                hidden.at[l, me], hidden.at[l, me], ag_ss, ag_rs.at[wave_of[m]], 2 * chip_of[m] + other
            ).start()

    for q in range(4):
        forward_wave(layers - 1, q)
    for q in range(4):
        whole(layers - 1, q)
    for j in range(n):
        tokens_out[:, j * LANES : (j + 1) * LANES] = hidden[layers - 1, j]
    sent(rs_send.at[layers - 1], rs_ss)
    sent(blocks(layers - 1, chips), ag_ss)
    sent(blocks(layers - 1, chips - 1), fw_ss)


def flush(tokens, state, value, key, tokens_hbm, state_hbm, value_hbm, key_hbm, sems):
    layers, batch = state.shape[:2]
    step = batch // 4
    copies = [
        pltpu.make_async_copy(key, key_hbm, sems.at[0]),
        pltpu.make_async_copy(value, value_hbm, sems.at[1]),
        pltpu.make_async_copy(tokens, tokens_hbm, sems.at[2]),
    ]
    for l in range(layers):
        for i in range(4):
            at = pl.ds(i * step, step)
            copies.append(
                pltpu.make_async_copy(state.at[l, at], state_hbm.at[l, at], sems.at[len(copies)])
            )
    for copy in copies:
        copy.start()
    for copy in copies:
        copy.wait()


def fused(n, *args):
    (tokens, norm_gain, w_gate, w_value, w_write, w_read, w_step, step_bias, decay_rate) = args[:9]
    (skip_gain, cvw, ckw, group_gain, w_out, ssm_state, conv_value, conv_key) = args[9:]
    layers, batch, chans, entries = ssm_state.shape
    depth = tokens.shape[1]
    chips = n // 2
    key_cols = w_write.shape[2]
    operands = list(args)
    operands[4] = jnp.swapaxes(w_write, 1, 2)
    operands[5] = jnp.swapaxes(w_read, 1, 2)
    operands[10] = jnp.swapaxes(cvw, 0, 1)
    landed = [pltpu.VMEM(a.shape, a.dtype) for a in operands]
    landed[4:6] = [pltpu.VMEM((layers, 2 * key_cols, depth), BF16)]
    del landed[13]
    dma = pltpu.SemaphoreType.DMA
    outs = (
        jax.ShapeDtypeStruct(tokens.shape, BF16),
        jax.ShapeDtypeStruct(ssm_state.shape, F32),
        jax.ShapeDtypeStruct(conv_value.shape, F32),
        jax.ShapeDtypeStruct(conv_key.shape, F32),
    )
    small_bytes = 4 * 1024 * 1024
    results = pl.pallas_call(
        functools.partial(mixer, n),
        out_shape=tuple(pltpu.VMEM(o.shape, o.dtype) for o in outs),
        in_specs=[pl.BlockSpec(memory_space=pltpu.HBM)] * len(operands),
        out_specs=(pl.BlockSpec(memory_space=pltpu.VMEM),) * 4,
        scratch_shapes=landed
        + [
            pltpu.VMEM((layers, n, batch, LANES), BF16),
            pltpu.VMEM((chips, batch, depth // chips), BF16),
            pltpu.VMEM((layers, GROUPS, 2, LANES), F32),
            pltpu.VMEM((layers, n, 2, LANES), F32),
            pltpu.VMEM((layers, chips, batch, LANES), BF16),
            pltpu.VMEM((layers, chips, batch, LANES), BF16),
            pltpu.VMEM((chips, batch, LANES), F32),
            pltpu.VMEM((layers, chips, batch, LANES), BF16),
            pltpu.VMEM((layers, chips, batch, LANES), BF16),
            pltpu.VMEM((layers, 1, LANES), F32),
            pltpu.VMEM((layers, 1, LANES), F32),
            pltpu.VMEM((layers, 1, LANES), F32),
            pltpu.VMEM((layers, chips, 1, LANES), F32),
            pltpu.VMEM((GROUPS, batch, LANES), F32),
            pltpu.VMEM((batch, entries, chans), BF16),
            pltpu.VMEM((chans, LANES), F32),
            pltpu.VMEM((batch, entries), F32),
            dma((17,)),
            dma((7,)),
            dma((4,)),
            dma((4,)),
            dma((4,)),
            dma((4,)),
        ],
        compiler_params=pltpu.CompilerParams(
            collective_id=0,
            has_side_effects=True,
            vmem_limit_bytes=VMEM - ssm_state.size * 4 - small_bytes,
        ),
        name="mixer",
    )(*operands)
    return pl.pallas_call(
        flush,
        out_shape=outs,
        in_specs=[pl.BlockSpec(memory_space=pl.ANY)] * 4,
        out_specs=(pl.BlockSpec(memory_space=pltpu.HBM),) * 4,
        scratch_shapes=[dma((3 + 4 * layers,))],
        compiler_params=pltpu.CompilerParams(vmem_limit_bytes=1024 * 1024),
        name="flush",
    )(*results)


def dispatch(n, *args):
    depth = args[0].shape[1]
    layers, batch, chans, entries = args[14].shape
    own_entries = args[4].shape[2] // GROUPS
    fits = (
        depth == n * LANES
        and n == 32
        and own_entries == 4
        and own_entries * batch == LANES
        and entries == LANES
        and chans == 2 * LANES
        and args[7].shape[1] == LANES
    )
    return fused(n, *args) if fits else per_device(*args)


def solution(mesh):
    placed = (
        P(),
        P(),
        P(None, None, "tp"),
        P(None, None, "tp"),
        P(None, None, "tp"),
        P(None, None, "tp"),
        P(),
        P(),
        P(),
        P(),
        P(None, None, "tp"),
        P(None, None, None, "tp"),
        P(None, "tp"),
        P(None, "tp", None),
        P(None, None, "tp", None),
        P(None, None, None, "tp"),
        P(None, None, None, None, "tp"),
    )
    return jax.shard_map(
        functools.partial(dispatch, mesh.shape["tp"]),
        mesh=mesh,
        in_specs=placed,
        out_specs=(
            P(),
            P(None, None, "tp", None),
            P(None, None, None, "tp"),
            P(None, None, None, None, "tp"),
        ),
        check_vma=False,
    )
```

```python
import jax
import jax.numpy as jnp
from jax import lax
from jax.experimental import pallas as pl
from jax.experimental.pallas import tpu as pltpu
from jax.sharding import PartitionSpec as P
import functools

D = 4096
HEAD_DIM = 64
GROUPS = 8
STATE = 128
LAYERS = 2
HEADS = 128
GW = 1024


EPS = 1e-06


def per_device(
    tokens,
    norm_gain,
    w_gate,
    w_value,
    w_write,
    w_read,
    w_step,
    step_bias,
    decay_rate,
    skip_gain,
    conv_value_weight,
    conv_key_weight,
    group_gain,
    w_out,
    ssm_state,
    conv_value,
    conv_key,
):
    highest = lax.Precision.HIGHEST
    chan_count = w_gate.shape[2]
    position = lax.axis_index("tp")
    first_chan = position * chan_count
    chan_ids = first_chan + jnp.arange(chan_count, dtype=jnp.int32)
    my_group = first_chan // GW
    head_hot = (
        (chan_ids // HEAD_DIM)[:, None] == jnp.arange(HEADS, dtype=jnp.int32)[None, :]
    ).astype(jnp.float32)
    group_hot = ((chan_ids // GW)[:, None] == jnp.arange(GROUPS, dtype=jnp.int32)[None, :]).astype(
        jnp.float32
    )
    hidden = tokens
    ssm_list = []
    value_list = []
    key_list = []
    for layer in range(LAYERS):
        resid = hidden.astype(jnp.float32)
        inv_scale = lax.rsqrt(jnp.sum(resid * resid, axis=1) / D + EPS)[:, None]
        scaled = (resid * norm_gain[layer]).astype(jnp.bfloat16)

        def project(weight):
            return jnp.dot(scaled, weight[layer], preferred_element_type=jnp.float32) * inv_scale

        gate_in = project(w_gate)
        value_in = project(w_value)
        write_in = project(w_write)
        read_in = project(w_read)
        step_in = project(w_step)
        value_window = jnp.concatenate([conv_value[layer], value_in[:, None, :]], axis=1)
        value_list.append(value_window[:, 1:])
        values = jax.nn.silu(jnp.sum(value_window * conv_value_weight[layer][None], axis=1))
        fresh = jnp.stack([write_in, read_in], axis=1)[:, None]
        key_window = jnp.concatenate([conv_key[layer], fresh], axis=1)
        key_list.append(key_window[:, 1:])
        mixed_keys = jax.nn.silu(jnp.sum(key_window * conv_key_weight[layer][None], axis=1))
        every_group = lax.all_gather(mixed_keys, "tp", axis=2, tiled=True)
        by_entry = every_group.reshape(every_group.shape[0], 2, STATE, GROUPS)
        own_keys = lax.dynamic_slice_in_dim(by_entry, my_group, 1, 3)[..., 0]
        writes = own_keys[:, 0]
        reads = own_keys[:, 1]
        delta = jax.nn.softplus(step_in + step_bias[layer][None])
        decay = jnp.exp(-delta * decay_rate[layer][None])
        delta_chan = jnp.dot(delta, head_hot.T, precision=highest)
        decay_chan = jnp.dot(decay, head_hot.T, precision=highest)
        skip_chan = jnp.dot(skip_gain[layer], head_hot.T, precision=highest)
        state = (
            decay_chan[..., None] * ssm_state[layer]
            + (delta_chan * values)[..., None] * writes[:, None, :]
        )
        ssm_list.append(state)
        read_out = jnp.sum(state * reads[:, None, :], axis=2) + skip_chan[None] * values
        gated = read_out * jax.nn.silu(gate_in)
        squares = jnp.dot(gated * gated, group_hot, precision=highest)
        square_total = lax.psum(squares, "tp")
        group_scale = lax.rsqrt(square_total / GW + EPS)
        scale_chan = jnp.dot(group_scale, group_hot.T, precision=highest)
        normed = (gated * scale_chan * group_gain[layer][None]).astype(jnp.bfloat16)
        partial_out = jnp.dot(normed, w_out[layer], preferred_element_type=jnp.float32)
        update = lax.psum(partial_out, "tp")
        hidden = (resid + update).astype(jnp.bfloat16)
    return (hidden, jnp.stack(ssm_list), jnp.stack(value_list), jnp.stack(key_list))


LANES = 128
TAPS = 3
VMEM = 67043328
BF16 = jnp.bfloat16
F32 = jnp.float32
NT = (((1,), (1,)), ((), ()))


def split3(x):
    high = x.astype(BF16)
    rest = x - high.astype(F32)
    mid = rest.astype(BF16)
    return high, mid, (rest - mid.astype(F32)).astype(BF16)


def select_dot(x, hot):
    rows = x.shape[0]
    parts = jnp.concatenate(split3(x), axis=0)
    out = jnp.dot(parts, hot, preferred_element_type=F32)
    return out[:rows] + out[rows : 2 * rows] + out[2 * rows :]


def silu(v):
    return v / (1.0 + jnp.exp(-v))


def iota(shape, axis):
    return lax.broadcasted_iota(jnp.int32, shape, axis)


def mixer(
    n,
    tokens_hbm,
    gain_hbm,
    wg_hbm,
    wv_hbm,
    ww_hbm,
    wr_hbm,
    ws_hbm,
    bias_hbm,
    rate_hbm,
    skip_hbm,
    cvw_hbm,
    ckw_hbm,
    gg_hbm,
    wo_hbm,
    state_hbm,
    cv_hbm,
    ck_hbm,
    tokens_out,
    state,
    value_out,
    key_out,
    tokens,
    gain,
    wg,
    wv,
    wk,
    ws,
    bias,
    rate,
    skip,
    cvw,
    ckw,
    gg,
    wo,
    cv,
    ck,
    hidden,
    scaled,
    keys_send,
    keys_recv,
    pair_send,
    pair_recv,
    part,
    rs_send,
    rs_recv,
    sq_own,
    sq_pair,
    sq_send,
    sq_recv,
    scales,
    turned,
    cols,
    wbuf,
    in_sem,
    send_sem,
    recv_sem,
    pair_rs,
    ag_rs,
    fw_rs,
):
    key_ss, pair_ss, rs_ss, ag_ss, fw_ss, sp_ss, sq_ss = [send_sem.at[i] for i in range(7)]
    key_rs, sp_rs, sq_rs, rs_rs = [recv_sem.at[i] for i in range(4)]
    layers, batch, chans, entries = state.shape
    depth = tokens.shape[1]
    chips = n // 2
    block = depth // chips
    key_cols = wk.shape[1] // 2
    own_entries = key_cols // GROUPS
    heads = bias.shape[1]
    peers = GW // chans
    per_group = peers // 2
    me = lax.axis_index("tp")
    chip = me // 2
    core = lax.rem(me, 2)
    other = 1 - core
    buddy = 2 * chip + other
    my_group = me // peers

    small_pairs = (
        (tokens_hbm, tokens),
        (gain_hbm, gain),
        (ck_hbm, ck),
        (ckw_hbm, ckw),
        (bias_hbm, bias),
        (rate_hbm, rate),
        (skip_hbm, skip),
        (cvw_hbm, cvw),
        (gg_hbm, gg),
        (cv_hbm, cv),
    )
    small = [pltpu.make_async_copy(a, b, in_sem.at[i]) for i, (a, b) in enumerate(small_pairs)]
    big = [
        [
            pltpu.make_async_copy(a.at[l], b.at[l], in_sem.at[len(small_pairs) + i])
            for i, (a, b) in enumerate(
                (
                    (ww_hbm, wk.at[:, :key_cols]),
                    (wr_hbm, wk.at[:, key_cols:]),
                    (wg_hbm, wg),
                    (wv_hbm, wv),
                    (ws_hbm, ws),
                    (state_hbm, state),
                    (wo_hbm, wo),
                )
            )
        ]
        for l in range(layers)
    ]
    def flipped(value, mask):
        bit = 1
        out = value
        while bit <= mask:
            if mask & bit:
                out = out + bit - 2 * bit * lax.rem(value // bit, 2)
            bit *= 2
        return out

    chip_of = [flipped(chip, m) for m in range(chips)]

    def distance(m):
        return (m >> 2) + (m >> 1) % 2 + m % 2

    far = sorted(range(chips), key=lambda m: (-distance(m), m))
    near = far[::-1]

    barrier = pltpu.get_barrier_semaphore()

    def signal(to):
        pl.semaphore_signal(barrier, inc=1, device_id=(to,), device_id_type=pl.DeviceIdType.MESH)

    for m in far[:4]:
        signal(2 * chip_of[m])
        signal(2 * chip_of[m] + 1)
    for copy in small[:4] + big[0][:2]:
        copy.start()
    for m in far[4:-1]:
        signal(2 * chip_of[m])
        signal(2 * chip_of[m] + 1)
    signal(buddy)

    def remote(src, dst, ss, rs, to):
        return pltpu.make_async_remote_copy(
            src_ref=src,
            dst_ref=dst,
            send_sem=ss,
            recv_sem=rs,
            device_id=(to,),
            device_id_type=pl.DeviceIdType.MESH,
        )

    senders = entries // own_entries
    row = iota((entries, entries), 0)
    col = iota((entries, entries), 1)
    natural = jnp.where(
        col == (row % senders) * own_entries + row // senders, 1.0, 0.0
    ).astype(BF16)
    row = iota((heads, chans), 0)
    col = iota((heads, chans), 1)
    head_hot = jnp.where(row == (me * chans + col) // HEAD_DIM, 1.0, 0.0).astype(BF16)

    groups8 = batch // 8

    def update_state(l, group):
        shifted = pltpu.roll(cols[...], lax.rem(LANES - 8 * group, LANES), 1)
        writes8 = wbuf[pl.ds(pl.multiple_of(8 * group, 8), 8), :]
        for j in range(8):
            b = 8 * group + j
            state[l, b] = (
                shifted[:, batch + j : batch + j + 1] * state[l, b]
                + shifted[:, j : j + 1] * writes8[j : j + 1, :]
            )

    def update_range(l, low, high):
        def step(g, carry):
            update_state(l, g)
            return carry

        lax.fori_loop(low, high, step, 0)

    def at_chip(c):
        return pl.ds(pl.multiple_of(c * block, block), block)

    def prepare(l, pos, c, squares):
        if l == 0:
            x = tokens[:, at_chip(c)].astype(F32)
        else:
            x = jnp.concatenate([hidden[l - 1, 2 * c], hidden[l - 1, 2 * c + 1]], axis=1).astype(F32)
        scaled[pos] = (x * gain[l : l + 1, at_chip(c)]).astype(BF16)
        return squares + x * x

    def key_dot(l, pos, c, acc):
        return acc + lax.dot_general(
            scaled[pos], wk[l, :, at_chip(c)], NT, preferred_element_type=F32
        )

    def main_dots(l, pos, c, accs):
        return tuple(
            acc + jnp.dot(scaled[pos], ref[l, at_chip(c), :], preferred_element_type=F32)
            for acc, ref in zip(accs, (wg, wv, ws))
        )

    def send_keys(l, key_acc, squares):
        inv_scale = lax.rsqrt(jnp.sum(squares, axis=1, keepdims=True) / depth + EPS)
        key_in = key_acc * inv_scale
        mixed = []
        for i in range(2):
            fresh = key_in[:, i * key_cols : (i + 1) * key_cols]
            total = fresh * ckw[l, TAPS - 1, i : i + 1, :]
            for k in range(TAPS - 1):
                total = total + ck[l, :, k, i, :] * ckw[l, k, i : i + 1, :]
            mixed.append(silu(total))
        mixed = jnp.concatenate(
            mixed + [jnp.zeros((batch, LANES - 2 * key_cols), F32)], axis=1
        )
        spread = jnp.concatenate([mixed] * own_entries, axis=0).T
        lane_entry = iota((GROUPS, LANES), 1) // batch
        for i in range(2):
            packed = jnp.zeros((GROUPS, LANES), F32)
            for e in range(own_entries):
                at = (i * own_entries + e) * GROUPS
                packed = jnp.where(lane_entry == e, spread[at : at + GROUPS], packed)
            keys_send[l, :, i, :] = packed
        keys_recv[l, me] = keys_send[l, my_group]
        if l == 0:
            pl.semaphore_wait(barrier, n - 1)
        for m in far:
            for to in ([2 * chip_of[m], 2 * chip_of[m] + 1] if m else [buddy]):
                remote(
                    keys_send.at[l, to // peers], keys_recv.at[l, me], key_ss, key_rs, to
                ).start()
        return inv_scale, key_in

    zeros = tuple(jnp.zeros((batch, ref.shape[2]), F32) for ref in (wg, wv, ws))
    key_zero = jnp.zeros((batch, 2 * key_cols), F32)
    square_zero = jnp.zeros((batch, block), F32)

    quarter = chips // 4
    waves = [near[q * quarter : (q + 1) * quarter] for q in range(4)]
    wave_of = {m: q for q, wave in enumerate(waves) for m in wave}

    def blocks(l, count):
        return hidden.at[l, pl.ds(0, count)]

    def forward_wave(l, q):
        remote(blocks(l, quarter), blocks(l, quarter), ag_ss, ag_rs.at[q], buddy).wait_recv()
        for m in waves[q]:
            if m:
                at = hidden.at[l, 2 * chip_of[m] + other]
                remote(at, at, fw_ss, fw_rs.at[q], buddy).start()

    def whole(l, q):
        count = sum(1 for m in waves[q] if m)
        remote(blocks(l, count), blocks(l, count), fw_ss, fw_rs.at[q], buddy).wait_recv()

    def sent(src, sem):
        remote(src, src, sem, rs_rs, buddy).wait_send()

    for l in range(layers):
        if l == 0:
            for copy in big[0][2:5] + small[4:]:
                copy.start()
            for copy in small[:4] + big[0][:2]:
                copy.wait()
            squares = square_zero
            key_acc = key_zero
            for c in range(chips):
                squares = prepare(l, c, c, squares)
                key_acc = key_dot(l, c, c, key_acc)
            inv_scale, key_in = send_keys(l, key_acc, squares)
            for copy in big[0][5:]:
                copy.start()
            for copy in big[0][2:5]:
                copy.wait()
            accs = zeros
            for c in range(chips):
                accs = main_dots(l, c, c, accs)
            for copy in small[4:]:
                copy.wait()
        else:
            for copy in big[l][:5]:
                copy.wait()
            squares, key_acc, accs = square_zero, key_zero, zeros
            for q in range(4):
                forward_wave(l - 1, q)
            for q, wave in enumerate(waves):
                whole(l - 1, q)
                for i, m in enumerate(wave):
                    pos = q * quarter + i
                    squares = prepare(l, pos, chip_of[m], squares)
                    key_acc = key_dot(l, pos, chip_of[m], key_acc)
            inv_scale, key_in = send_keys(l, key_acc, squares)
            for pos, m in enumerate(near):
                accs = main_dots(l, pos, chip_of[m], accs)
        gate_in, value_in, step_in = [acc * inv_scale for acc in accs]
        for i in range(2):
            for k in range(1, TAPS - 1):
                key_out[l, :, k - 1, i, :] = ck[l, :, k, i, :]
            key_out[l, :, TAPS - 2, i, :] = key_in[:, i * key_cols : (i + 1) * key_cols]
        for k in range(1, TAPS - 1):
            value_out[l, :, k - 1, :] = cv[l, :, k, :]
        value_out[l, :, TAPS - 2, :] = value_in
        values = value_in * cvw[TAPS - 1, l : l + 1, :]
        for k in range(TAPS - 1):
            values = values + cv[l, :, k, :] * cvw[k, l : l + 1, :]
        values = silu(values)
        raw = step_in + bias[l : l + 1, :]
        delta = jnp.maximum(raw, 0.0) + jnp.log1p(jnp.exp(-jnp.abs(raw)))
        decay = jnp.exp(-delta * rate[l : l + 1, :])
        skips = jnp.broadcast_to(skip[l : l + 1, :], (8, heads))
        chan = select_dot(jnp.concatenate([delta, decay, skips], axis=0), head_hot)
        decay_chan = chan[batch : 2 * batch]
        skip_chan = chan[2 * batch : 2 * batch + 1]
        dv = chan[:batch] * values
        cols[...] = jnp.concatenate(
            [dv, decay_chan, jnp.zeros((LANES - 2 * batch, chans), F32)], axis=0
        ).T
        gate = silu(gate_in)
        big[l][5].wait()
        if l:
            sent(rs_send.at[l - 1], rs_ss)
            sent(blocks(l - 1, chips), ag_ss)
            sent(blocks(l - 1, chips - 1), fw_ss)

        def turn(g, carry):
            for j in range(8):
                turned[8 * g + j] = lax.dot_general(
                    natural, state[l, 8 * g + j].astype(BF16), NT, preferred_element_type=F32
                ).astype(BF16)
            return carry

        lax.fori_loop(0, groups8, turn, 0)
        big[l][6].wait()

        remote(
            keys_recv.at[l, pl.ds(0, n - 1)], keys_recv.at[l, pl.ds(0, n - 1)],
            key_ss, key_rs, buddy,
        ).wait_recv()
        lane_entry = iota((batch, LANES), 1) // senders
        grouped = []
        for i in range(2):
            arrived = jnp.concatenate([keys_recv[l, :, i, :]] * own_entries, axis=0).T
            rows = arrived[:batch]
            for e in range(1, own_entries):
                rows = jnp.where(lane_entry == e, arrived[e * batch : (e + 1) * batch], rows)
            grouped.append(rows)
        writes, reads = grouped
        lane_half = iota((8, 2 * entries), 1) // entries
        sub = iota((8, 2 * entries), 0)
        query = []
        for g in range(groups8):
            reads8 = reads[8 * g : 8 * g + 8]
            twice = jnp.concatenate([reads8, reads8], axis=1)
            total = jnp.zeros((8, chans), F32)
            for p in range(4):
                left = jnp.where(sub == 2 * p + lane_half, twice, 0.0).astype(BF16)
                right = turned[pl.ds(8 * g + 2 * p, 2)].reshape(2 * entries, chans)
                total = total + jnp.dot(left, right, preferred_element_type=F32)
            query.append(total)
        query = jnp.concatenate(query, axis=0)
        through = jnp.sum(writes * reads, axis=1, keepdims=True)
        mixed_out = decay_chan * query + dv * through + skip_chan * values
        gated = mixed_out * gate
        fed = (gated * gg[l : l + 1, :]).astype(BF16)

        def out_pair(i, parity):
            rhs = jnp.concatenate(
                [
                    wo[l, :, pl.ds(pl.multiple_of((2 * chip_of[far[i + j]] + parity) * LANES, LANES), LANES)]
                    for j in range(2)
                ],
                axis=1,
            )
            return jnp.dot(fed, rhs, preferred_element_type=F32)

        square = gated * gated
        square = square[:, :LANES] + square[:, LANES:]
        square = jnp.concatenate([square, jnp.zeros((LANES - batch, LANES), F32)], axis=0).T
        sq_own[l] = jnp.sum(square, axis=0, keepdims=True)
        sp_copy = remote(sq_own.at[l], sq_pair.at[l], sp_ss, sp_rs, buddy)
        sp_copy.start()

        def pair_copy(q):
            at = pl.ds(q * quarter, quarter)
            return remote(pair_send.at[l, at], pair_recv.at[l, at], pair_ss, pair_rs.at[q], buddy)

        for q in range(4):
            for i in range(q * quarter, (q + 1) * quarter, 2):
                res = out_pair(i, core).astype(BF16)
                pair_send[l, i] = res[:, :LANES]
                pair_send[l, i + 1] = res[:, LANES:]
            pair_copy(q).start()
        for i in range(0, chips, 2):
            res = out_pair(i, other)
            part[i] = res[:, :LANES]
            part[i + 1] = res[:, LANES:]
        sp_copy.wait_recv()
        sq_send[l] = sq_own[l] + sq_pair[l]
        for m in far:
            remote(
                sq_send.at[l], sq_recv.at[l, chip], sq_ss, sq_rs, 2 * chip_of[m] + other
            ).start()

        def rs_copy(i):
            return remote(
                rs_send.at[l, i], rs_recv.at[l, chip], rs_ss, rs_rs, 2 * chip_of[far[i]] + other
            )

        for q in range(4):
            pair_copy(q).wait_recv()
            for i in range(q * quarter, (q + 1) * quarter):
                rs_send[l, i] = (part[i] + pair_recv[l, i].astype(F32)).astype(BF16)
                rs_copy(i).start()
        if l + 1 < layers:
            for copy in big[l + 1]:
                copy.start()
        wbuf[...] = select_dot(writes, natural)
        update_range(l, 0, groups8)
        sent(keys_recv.at[l, pl.ds(0, n - 1)], key_ss)
        sent(sq_own.at[l], sp_ss)
        sent(pair_send.at[l], pair_ss)
        sent(sq_recv.at[l], sq_ss)
        remote(sq_recv.at[l], sq_recv.at[l], sq_ss, sq_rs, buddy).wait_recv()
        rows = []
        for g in range(GROUPS):
            total = sq_recv[l, per_group * g]
            for k in range(1, per_group):
                total = total + sq_recv[l, per_group * g + k]
            rows.append(total)
        rows = lax.rsqrt(jnp.concatenate(rows, axis=0) / GW + EPS)
        columns = jnp.concatenate([rows, jnp.zeros((LANES - GROUPS, LANES), F32)], axis=0).T
        for g in range(GROUPS):
            scales[g] = jnp.broadcast_to(columns[:batch, g : g + 1], (batch, LANES))
        if l == 0:
            resid = tokens[:, pl.ds(pl.multiple_of(me * LANES, LANES), LANES)]
        else:
            resid = hidden[l - 1, me]
        remote(rs_recv.at[l], rs_recv.at[l], rs_ss, rs_rs, buddy).wait_recv()
        sums = [resid.astype(F32)] + [jnp.zeros((batch, LANES), F32)] * 3
        for g in range(GROUPS):
            term = rs_recv[l, per_group * g].astype(F32)
            for k in range(1, per_group):
                term = term + rs_recv[l, per_group * g + k].astype(F32)
            sums[g % 4] = sums[g % 4] + term * scales[g]
        hidden[l, me] = ((sums[0] + sums[1]) + (sums[2] + sums[3])).astype(BF16)
        for m in far:
            remote(
                hidden.at[l, me], hidden.at[l, me], ag_ss, ag_rs.at[wave_of[m]], 2 * chip_of[m] + other
            ).start()

    for q in range(4):
        forward_wave(layers - 1, q)
    for q in range(4):
        whole(layers - 1, q)
    for j in range(n):
        tokens_out[:, j * LANES : (j + 1) * LANES] = hidden[layers - 1, j]
    sent(rs_send.at[layers - 1], rs_ss)
    sent(blocks(layers - 1, chips), ag_ss)
    sent(blocks(layers - 1, chips - 1), fw_ss)


def flush(tokens, state, value, key, tokens_hbm, state_hbm, value_hbm, key_hbm, sems):
    layers, batch = state.shape[:2]
    step = batch // 4
    copies = [
        pltpu.make_async_copy(key, key_hbm, sems.at[0]),
        pltpu.make_async_copy(value, value_hbm, sems.at[1]),
        pltpu.make_async_copy(tokens, tokens_hbm, sems.at[2]),
    ]
    for l in range(layers):
        for i in range(4):
            at = pl.ds(i * step, step)
            copies.append(
                pltpu.make_async_copy(state.at[l, at], state_hbm.at[l, at], sems.at[len(copies)])
            )
    for copy in copies[3:] + copies[:3]:
        copy.start()
    for copy in copies:
        copy.wait()


def fused(n, *args):
    (tokens, norm_gain, w_gate, w_value, w_write, w_read, w_step, step_bias, decay_rate) = args[:9]
    (skip_gain, cvw, ckw, group_gain, w_out, ssm_state, conv_value, conv_key) = args[9:]
    layers, batch, chans, entries = ssm_state.shape
    depth = tokens.shape[1]
    chips = n // 2
    key_cols = w_write.shape[2]
    operands = list(args)
    operands[4] = jnp.swapaxes(w_write, 1, 2)
    operands[5] = jnp.swapaxes(w_read, 1, 2)
    operands[10] = jnp.swapaxes(cvw, 0, 1)
    landed = [pltpu.VMEM(a.shape, a.dtype) for a in operands]
    landed[4:6] = [pltpu.VMEM((layers, 2 * key_cols, depth), BF16)]
    del landed[13]
    dma = pltpu.SemaphoreType.DMA
    outs = (
        jax.ShapeDtypeStruct(tokens.shape, BF16),
        jax.ShapeDtypeStruct(ssm_state.shape, F32),
        jax.ShapeDtypeStruct(conv_value.shape, F32),
        jax.ShapeDtypeStruct(conv_key.shape, F32),
    )
    small_bytes = 4 * 1024 * 1024
    results = pl.pallas_call(
        functools.partial(mixer, n),
        out_shape=tuple(pltpu.VMEM(o.shape, o.dtype) for o in outs),
        in_specs=[pl.BlockSpec(memory_space=pltpu.HBM)] * len(operands),
        out_specs=(pl.BlockSpec(memory_space=pltpu.VMEM),) * 4,
        scratch_shapes=landed
        + [
            pltpu.VMEM((layers, n, batch, LANES), BF16),
            pltpu.VMEM((chips, batch, depth // chips), BF16),
            pltpu.VMEM((layers, GROUPS, 2, LANES), F32),
            pltpu.VMEM((layers, n, 2, LANES), F32),
            pltpu.VMEM((layers, chips, batch, LANES), BF16),
            pltpu.VMEM((layers, chips, batch, LANES), BF16),
            pltpu.VMEM((chips, batch, LANES), F32),
            pltpu.VMEM((layers, chips, batch, LANES), BF16),
            pltpu.VMEM((layers, chips, batch, LANES), BF16),
            pltpu.VMEM((layers, 1, LANES), F32),
            pltpu.VMEM((layers, 1, LANES), F32),
            pltpu.VMEM((layers, 1, LANES), F32),
            pltpu.VMEM((layers, chips, 1, LANES), F32),
            pltpu.VMEM((GROUPS, batch, LANES), F32),
            pltpu.VMEM((batch, entries, chans), BF16),
            pltpu.VMEM((chans, LANES), F32),
            pltpu.VMEM((batch, entries), F32),
            dma((17,)),
            dma((7,)),
            dma((4,)),
            dma((4,)),
            dma((4,)),
            dma((4,)),
        ],
        compiler_params=pltpu.CompilerParams(
            collective_id=0,
            has_side_effects=True,
            vmem_limit_bytes=VMEM - ssm_state.size * 4 - small_bytes,
        ),
        name="mixer",
    )(*operands)
    return pl.pallas_call(
        flush,
        out_shape=outs,
        in_specs=[pl.BlockSpec(memory_space=pl.ANY)] * 4,
        out_specs=(pl.BlockSpec(memory_space=pltpu.HBM),) * 4,
        scratch_shapes=[dma((3 + 4 * layers,))],
        compiler_params=pltpu.CompilerParams(vmem_limit_bytes=1024 * 1024),
        name="flush",
    )(*results)


def dispatch(n, *args):
    depth = args[0].shape[1]
    layers, batch, chans, entries = args[14].shape
    own_entries = args[4].shape[2] // GROUPS
    fits = (
        depth == n * LANES
        and n == 32
        and own_entries == 4
        and own_entries * batch == LANES
        and entries == LANES
        and chans == 2 * LANES
        and args[7].shape[1] == LANES
    )
    return fused(n, *args) if fits else per_device(*args)


def solution(mesh):
    placed = (
        P(),
        P(),
        P(None, None, "tp"),
        P(None, None, "tp"),
        P(None, None, "tp"),
        P(None, None, "tp"),
        P(),
        P(),
        P(),
        P(),
        P(None, None, "tp"),
        P(None, None, None, "tp"),
        P(None, "tp"),
        P(None, "tp", None),
        P(None, None, "tp", None),
        P(None, None, None, "tp"),
        P(None, None, None, None, "tp"),
    )
    return jax.shard_map(
        functools.partial(dispatch, mesh.shape["tp"]),
        mesh=mesh,
        in_specs=placed,
        out_specs=(
            P(),
            P(None, None, "tp", None),
            P(None, None, None, "tp"),
            P(None, None, None, None, "tp"),
        ),
        check_vma=False,
    )
```
